1024 devices in a mesh: dp: 8 (over x), kv: 64 (over z, y), tp: 2 (over core).
Axes of the slice: x: 8, y: 8, z: 8, core: 2. Of those that a mesh axis runs over, the one named last changes fastest.
Arguments:
- piece_tokens: bfloat16 [8192, 2048], P(('dp', 'kv')), parts along dimension 0, may hold values from -6 to 6
- dec_tokens: bfloat16 [6144, 4, 2048], P(('dp', 'kv')), parts along dimension 0, may hold values from -6 to 6
- norm_gain: float32 [2048], replicated, may hold values from 0.1 to 1.9
- query_weight: bfloat16 [2048, 1024], P(None, 'tp'), may hold values from -0.375 to 0.375
- key_weight: bfloat16 [2048, 256], P(None, 'tp'), may hold values from -0.125 to 0.125
- value_weight: bfloat16 [2048, 256], P(None, 'tp'), may hold values from -0.125 to 0.125
- gate_weight: bfloat16 [2048, 8], P(None, 'tp'), may hold values from -0.125 to 0.125
- gate_bias: float32 [8], P('tp'), may hold values from 3.4 to 11
- out_weight: bfloat16 [1024, 2048], P('tp'), may hold values from -0.1875 to 0.1875
- out_gain: float32 [2048], replicated, may hold values from 0.1 to 1.9
- past_keys: bfloat16 [131072, 2, 128], P(('dp', 'kv'), 'tp'), parts along dimension 0, may hold values from -41 to 41
- past_values: bfloat16 [131072, 2, 128], P(('dp', 'kv'), 'tp'), parts along dimension 0, may hold values from -6 to 6
- past_gate: float32 [8, 131072], P('tp', ('dp', 'kv')), parts along dimension 1, may hold values from -16384 to 0
- dec_keys: bfloat16 [6144, 512, 2, 128], P(('dp', 'kv'), None, 'tp'), parts along dimension 0, may hold values from -41 to 41
- dec_values: bfloat16 [6144, 512, 2, 128], P(('dp', 'kv'), None, 'tp'), parts along dimension 0, may hold values from -6 to 6
- dec_gate: float32 [6144, 8, 512], P(('dp', 'kv'), 'tp'), parts along dimension 0, may hold values from -512 to 0
- dec_lengths: int32 [6144], P(('dp', 'kv')), parts along dimension 0, may hold values from 1 to 512, as said below
Outputs:
- piece_out: bfloat16 [8192, 2048], P(('dp', 'kv')), parts along dimension 0
- dec_out: bfloat16 [6144, 4, 2048], P(('dp', 'kv')), parts along dimension 0
The draws below stay inside these ranges and needn't reach their ends.
There are 8 independent parts, one for each index of `dp`. The reference program is written for one: setup_inputs(seed, part) draws one part's arguments, and reference() takes and returns one part's arrays. A program takes and returns all parts, laid end to end along the dimension named above; an argument that names none is the same for every part. Nothing has to cross between parts.
Inputs may be any that keep to these rules, and one draw needn't show every extreme that they name: `dec_lengths`: some decoding sequence has all 512 slots live in every draw.
All inputs are finite; a program needn't handle non-finite values.
Results may differ from the reference program's by a relative error of at most 0.015.
Values may be sent and summed in bfloat16 or wider, within the bound.
No kernel may reach another device: no remote copies, remote signals or barrier semaphores. Data moves between devices by JAX's collectives and lax.ppermute only.
A program may use at most 64 MiB of HBM per device.

```python
import math
import jax
import jax.numpy as jnp
from jax import lax

D = 2048
QUERY_HEADS = 8
KV_HEADS = 2
HEAD_DIM = 128
PAST_DEV = 256
DEC_NEW = 4
DEC_PAST = 512
PIECE = 1024
PAST = 16384
DEC_SEQS = 768
N_TP = 2


def fast_number():
    return QUERY_HEADS // 2


def head_rank(key):
    return jax.random.permutation(jax.random.fold_in(key, 11), QUERY_HEADS)


def gate_rates(key, leading_shape, length_total, block_len, fast_count):
    complete_shape = leading_shape + (QUERY_HEADS, length_total)
    fast_heads = (head_rank(key) < fast_count)[:, None]
    blocks = length_total // block_len
    factor = jnp.exp(jax.random.uniform(jax.random.fold_in(key, 12), leading_shape + (QUERY_HEADS, blocks), jnp.float32, 0.0, math.log(4.0)))
    factor = jnp.repeat(factor, block_len, axis=-1)
    jitter = jnp.exp(jax.random.uniform(jax.random.fold_in(key, 13), complete_shape, jnp.float32, -0.7, 0.7))
    fast_rate = 1.0 / (30.0 + 70.0 * jax.random.uniform(jax.random.fold_in(key, 14), leading_shape + (QUERY_HEADS, 1), jnp.float32))
    stable_value = jnp.where(fast_heads, fast_rate, 0.35 / length_total) * factor * jitter
    outlier_place = jax.random.randint(jax.random.fold_in(key, 15), leading_shape + (QUERY_HEADS, 3), 0, length_total)
    outlier_hit = jnp.any(jnp.arange(length_total) == outlier_place[..., None], axis=-2)
    outlier_size = jnp.where(outlier_hit, jax.random.uniform(jax.random.fold_in(key, 16), complete_shape, jnp.float32, 0.22, 0.45), 0.0)
    return -(stable_value + outlier_size)


def live_lengths(key):
    base_key = jax.random.fold_in(key, 41)
    first_draw = jax.random.randint(jax.random.fold_in(base_key, 1), (DEC_SEQS,), 1, DEC_PAST + 1)
    second_draw = jax.random.randint(jax.random.fold_in(base_key, 2), (DEC_SEQS,), 1, DEC_PAST + 1)
    product = jnp.maximum(first_draw * second_draw // DEC_PAST, 1)
    chosen = jax.random.randint(jax.random.fold_in(base_key, 3), (), 0, DEC_SEQS)
    return jnp.where(jnp.arange(DEC_SEQS) == chosen, DEC_PAST, product).astype(jnp.int32)


def draw_gate_bias(key, part):
    fast_heads = head_rank(key) < fast_number()
    spread = jax.random.uniform(jax.random.fold_in(key, 12), (QUERY_HEADS,), jnp.float32)
    return jnp.where(fast_heads, 3.4 + 1.2 * spread, 9.5 + 1.5 * spread)


def draw_past_keys(key, part):
    noise_rows = jnp.clip(jax.random.normal(jax.random.fold_in(key, 31), (PAST, KV_HEADS, HEAD_DIM), jnp.float32), -6.0, 6.0)
    return noise_rows.astype(jnp.bfloat16)


def draw_past_values(key, part):
    noise_rows = jax.random.normal(jax.random.fold_in(key, 37), (PAST, KV_HEADS, HEAD_DIM), jnp.float32)
    return jnp.clip(noise_rows, -6.0, 6.0).astype(jnp.bfloat16)


def draw_past_gate(key, part):
    gate_step = gate_rates(key, (), PAST, PAST_DEV, fast_number())
    return jnp.flip(jnp.cumsum(jnp.flip(gate_step, -1), -1), -1) - gate_step


def draw_dec_keys(key, part):
    noise_rows = jnp.clip(jax.random.normal(jax.random.fold_in(key, 34), (DEC_SEQS, DEC_PAST, KV_HEADS, HEAD_DIM), jnp.float32), -6.0, 6.0)
    return noise_rows.astype(jnp.bfloat16)


def draw_dec_gate(key, part):
    return jnp.cumsum(gate_rates(key, (DEC_SEQS,), DEC_PAST, DEC_PAST // 4, fast_number()), -1)


def draw_dec_lengths(key, part):
    return live_lengths(key)


def shard_levels(rng, shape, split, least, largest):
    loudness = 1.0
    for axis_at, parts in split:
        steps = jax.random.uniform(jax.random.fold_in(jax.random.fold_in(rng, 6), axis_at), (parts,), jnp.float32, least / len(split), largest / len(split))
        loudness = loudness * jnp.repeat(jnp.exp(steps), shape[axis_at] // parts).reshape((-1,) + (1,) * (len(shape) - 1 - axis_at))
    return loudness


def noise(stream_key, shape, scale, limit, cuts=(), kind=jnp.bfloat16):
    factor_of = shard_levels(stream_key, shape, cuts, -0.22, 0.18) if cuts else 1.0
    drawn = jax.random.normal(stream_key, shape, jnp.float32) * scale * factor_of
    return jnp.minimum(jnp.maximum(drawn, -limit), limit).astype(kind)


def setup_inputs(seed: int = 0, part: int = 0) -> dict:
    key_list = jax.random.split(jax.random.key(seed), 18)
    part_splits = jax.random.split(jax.random.fold_in(key_list[17], part), 18)
    piece_tokens = noise(part_splits[0], (PIECE, D), 1.0, 6.0, ((0, 64),))
    dec_tokens = noise(part_splits[1], (DEC_SEQS, DEC_NEW, D), 1.0, 6.0, ((0, 64),))
    norm_gain = jnp.clip(1.0 + 0.18 * jax.random.normal(key_list[2], (D,), jnp.float32), 0.1, 1.9)
    query_weight = noise(key_list[3], (D, QUERY_HEADS * HEAD_DIM), (D // 9) ** -0.5, 0.375, ((1, 2),))
    key_weight = noise(key_list[4], (D, KV_HEADS * HEAD_DIM), D ** -0.5, 0.125, ((1, 2),))
    value_weight = noise(key_list[5], (D, KV_HEADS * HEAD_DIM), D ** -0.5, 0.125, ((1, 2),))
    gate_weight = noise(key_list[6], (D, QUERY_HEADS), D ** -0.5, 0.125, ((1, 2),))
    gate_bias = draw_gate_bias(jax.random.fold_in(key_list[17], 71), part)
    out_weight = noise(key_list[8], (QUERY_HEADS * HEAD_DIM, D), (QUERY_HEADS * HEAD_DIM) ** -0.5, 0.1875, ((0, 2),))
    out_gain = jnp.clip(1.0 + 0.18 * jax.random.normal(key_list[9], (D,), jnp.float32), 0.1, 1.9)
    past_keys = draw_past_keys(jax.random.fold_in(jax.random.fold_in(key_list[17], part), 71), part)
    past_values = draw_past_values(jax.random.fold_in(jax.random.fold_in(key_list[17], part), 71), part)
    past_gate = draw_past_gate(jax.random.fold_in(jax.random.fold_in(key_list[17], part), 71), part)
    dec_keys = draw_dec_keys(jax.random.fold_in(jax.random.fold_in(key_list[17], part), 71), part)
    dec_values = noise(part_splits[14], (DEC_SEQS, DEC_PAST, KV_HEADS, HEAD_DIM), 1.0, 6.0, ((0, 64), (2, 2)))
    dec_gate = draw_dec_gate(jax.random.fold_in(jax.random.fold_in(key_list[17], part), 71), part)
    dec_lengths = draw_dec_lengths(jax.random.fold_in(jax.random.fold_in(key_list[17], part), 71), part)
    return dict(piece_tokens=piece_tokens, dec_tokens=dec_tokens, norm_gain=norm_gain, query_weight=query_weight, key_weight=key_weight, value_weight=value_weight, gate_weight=gate_weight, gate_bias=gate_bias, out_weight=out_weight, out_gain=out_gain, past_keys=past_keys, past_values=past_values, past_gate=past_gate, dec_keys=dec_keys, dec_values=dec_values, dec_gate=dec_gate, dec_lengths=dec_lengths)


EPS = 1e-06

def rms_scale(source, scale_gain):
    widened = source.astype(jnp.float32)
    return widened * lax.rsqrt(lax.optimization_barrier(jnp.mean(widened * widened, axis=-1, keepdims=True)) + EPS) * scale_gain

def attend(scores, value_block):
    row_top = lax.optimization_barrier(jnp.max(scores, axis=-1, keepdims=True))
    exponent = jnp.exp(scores - row_top)
    weights = exponent.astype(jnp.bfloat16)
    summed = jnp.einsum('gqk,kd->gqd', weights.astype(jnp.float32), value_block.astype(jnp.float32))
    return summed / lax.optimization_barrier(jnp.sum(exponent, axis=-1, keepdims=True))

def reference(piece_tokens, dec_tokens, norm_gain, query_weight, key_weight, value_weight, gate_weight, gate_bias, out_weight, out_gain, past_keys, past_values, past_gate, dec_keys, dec_values, dec_gate, dec_lengths):
    group_size = QUERY_HEADS // KV_HEADS
    score_scale = HEAD_DIM ** (-0.5)
    all_rows = jnp.concatenate([piece_tokens, dec_tokens.reshape(DEC_SEQS * DEC_NEW, D)], axis=0)
    normed = rms_scale(all_rows, norm_gain).astype(jnp.bfloat16)
    queries = jnp.dot(normed, query_weight, preferred_element_type=jnp.float32).astype(jnp.bfloat16)
    key_rows = jnp.dot(normed, key_weight, preferred_element_type=jnp.float32).astype(jnp.bfloat16)
    value_rows = jnp.dot(normed, value_weight, preferred_element_type=jnp.float32).astype(jnp.bfloat16)
    log_gates = jax.nn.log_sigmoid(jnp.dot(normed, gate_weight, preferred_element_type=jnp.float32) + gate_bias)
    piece_queries = queries[:PIECE].reshape(PIECE, KV_HEADS, group_size, HEAD_DIM)
    piece_run = jnp.cumsum(log_gates[:PIECE], axis=0)
    joined_keys = jnp.concatenate([past_keys, key_rows[:PIECE].reshape(PIECE, KV_HEADS, HEAD_DIM)], axis=0).astype(jnp.float32)
    joined_values = jnp.concatenate([past_values, value_rows[:PIECE].reshape(PIECE, KV_HEADS, HEAD_DIM)], axis=0)
    key_bias = jnp.concatenate([past_gate, -piece_run.T], axis=1).reshape(KV_HEADS, group_size, PAST + PIECE)
    block_rows = math.gcd(PIECE, 64)
    key_index = jnp.arange(PAST + PIECE)

    def piece_block(block_start):
        block_queries = lax.dynamic_slice_in_dim(piece_queries, block_start, block_rows, 0).astype(jnp.float32)
        block_run = lax.dynamic_slice_in_dim(piece_run, block_start, block_rows, 0).reshape(block_rows, KV_HEADS, group_size)
        row_place = block_start + jnp.arange(block_rows)
        visible = key_index[None, :] <= PAST + row_place[:, None]
        results = []
        for kv_head in range(KV_HEADS):
            scores = jnp.einsum('bgd,kd->gbk', block_queries[:, kv_head], joined_keys[:, kv_head]) * score_scale
            scores = scores + key_bias[kv_head][:, None, :] + block_run[:, kv_head].T[:, :, None]
            scores = jnp.where(visible[None], scores, -jnp.inf)
            results.append(attend(scores, joined_values[:, kv_head]))
        return jnp.stack(results, axis=0)
    starts = (jnp.arange(PIECE // block_rows) * block_rows).astype(jnp.int32)
    piece_blocks = lax.map(piece_block, starts)
    piece_attention = jnp.transpose(piece_blocks, (0, 3, 1, 2, 4)).reshape(PIECE, QUERY_HEADS * HEAD_DIM).astype(jnp.bfloat16)
    dec_queries = queries[PIECE:].reshape(DEC_SEQS, DEC_NEW, KV_HEADS, group_size, HEAD_DIM)
    dec_new_keys = key_rows[PIECE:].reshape(DEC_SEQS, DEC_NEW, KV_HEADS, HEAD_DIM)
    dec_new_values = value_rows[PIECE:].reshape(DEC_SEQS, DEC_NEW, KV_HEADS, HEAD_DIM)
    dec_run = jnp.cumsum(log_gates[PIECE:].reshape(DEC_SEQS, DEC_NEW, QUERY_HEADS), axis=1)
    slot_index = jnp.arange(DEC_PAST + DEC_NEW)
    new_index = jnp.arange(DEC_NEW)

    def dec_sequence(inputs):
        seq_queries, new_keys, new_values, seq_run, old_keys, old_values, old_gate, length_total = inputs
        last_gate = lax.dynamic_slice_in_dim(old_gate, (length_total - 1).astype(jnp.int32), 1, 1)[:, 0]
        joined = jnp.concatenate([old_keys, new_keys], axis=0).astype(jnp.float32)
        joined_rows = jnp.concatenate([old_values, new_values], axis=0)
        seq_bias = jnp.concatenate([last_gate[:, None] - old_gate, -seq_run.T], axis=1)
        seq_bias = seq_bias.reshape(KV_HEADS, group_size, DEC_PAST + DEC_NEW)
        visible = jnp.where(slot_index[None, :] < DEC_PAST, slot_index[None, :] < length_total, slot_index[None, :] - DEC_PAST <= new_index[:, None])
        row_bias = seq_run.reshape(DEC_NEW, KV_HEADS, group_size)
        results = []
        for kv_head in range(KV_HEADS):
            scores = jnp.einsum('tgd,kd->gtk', seq_queries[:, kv_head].astype(jnp.float32), joined[:, kv_head]) * score_scale
            scores = scores + seq_bias[kv_head][:, None, :] + row_bias[:, kv_head].T[:, :, None]
            scores = jnp.where(visible[None], scores, -jnp.inf)
            results.append(attend(scores, joined_rows[:, kv_head]))
        return jnp.stack(results, axis=0)
    dec_blocks = lax.map(dec_sequence, (dec_queries, dec_new_keys, dec_new_values, dec_run, dec_keys, dec_values, dec_gate, dec_lengths))
    dec_attention = jnp.transpose(dec_blocks, (0, 3, 1, 2, 4)).reshape(DEC_SEQS * DEC_NEW, QUERY_HEADS * HEAD_DIM).astype(jnp.bfloat16)
    attention = jnp.concatenate([piece_attention, dec_attention], axis=0)
    group_width = QUERY_HEADS * HEAD_DIM // N_TP
    mixed = jnp.zeros((attention.shape[0], D), jnp.float32)
    for tp_group in range(N_TP):
        head_partial = jnp.dot(attention[:, tp_group * group_width:(tp_group + 1) * group_width], out_weight[tp_group * group_width:(tp_group + 1) * group_width], preferred_element_type=jnp.float32).astype(jnp.bfloat16)
        mixed = mixed + lax.optimization_barrier(head_partial).astype(jnp.float32)
    final_rows = rms_scale(mixed, out_gain).astype(jnp.bfloat16)
    return (final_rows[:PIECE], final_rows[PIECE:].reshape(DEC_SEQS, DEC_NEW, D))
```

```python
import functools

import jax
import jax.numpy as jnp
from jax import lax
from jax.experimental import pallas as pl
from jax.experimental.pallas import tpu as pltpu
from jax.sharding import Mesh
from jax.sharding import PartitionSpec as P

KV = ("zh", "zl", "y")
NEAR = ("zl", "y")
DP_KV = ("dp", "zh", "zl", "y")
EPS = 1e-06
LANES = 128
F32 = jnp.float32
BF16 = jnp.bfloat16


def rms_scale(source, scale_gain):
    widened = source.astype(F32)
    return (
        widened * lax.rsqrt(jnp.mean(widened * widened, axis=-1, keepdims=True) + EPS) * scale_gain
    )


def three_parts(x):
    high = x.astype(BF16).astype(F32)
    rest = x - high
    middle = rest.astype(BF16).astype(F32)
    low = (rest - middle).astype(BF16).astype(F32)
    return high, middle, low


def lane_index(shape):
    return lax.broadcasted_iota(jnp.int32, shape, len(shape) - 1)


def row_index(shape):
    return lax.broadcasted_iota(jnp.int32, shape, 0)


def pack_lanes(x, heads):
    high, middle, low = three_parts(x)
    lane = lane_index(x.shape)
    middle = pltpu.roll(middle, heads, 1)
    low = pltpu.roll(low, 2 * heads, 1)
    return jnp.where(
        lane < heads,
        high,
        jnp.where(lane < 2 * heads, middle, jnp.where(lane < 3 * heads, low, 0.0)),
    )


def unpack_lanes(x, heads):
    return x + pltpu.roll(x, LANES - heads, 1) + pltpu.roll(x, LANES - 2 * heads, 1)


def proj_kernel(
    heads,
    tok_hbm,
    gain_ref,
    wq_hbm,
    wk_hbm,
    wv_hbm,
    wg_hbm,
    bias_ref,
    share_ref,
    new_ref,
    run_ref,
    tok_ref,
    wq_ref,
    wk_ref,
    wv_ref,
    wg_ref,
    sems,
):
    copies = []
    for n, (src, dst) in enumerate(
        (
            (tok_hbm, tok_ref),
            (wg_hbm, wg_ref),
            (wk_hbm, wk_ref),
            (wv_hbm, wv_ref),
            (wq_hbm, wq_ref),
        )
    ):
        copy = pltpu.make_async_copy(src, dst, sems.at[n])
        copy.start()
        copies.append(copy)
    copies[0].wait()
    normed = rms_scale(tok_ref[...], gain_ref[...]).astype(BF16)
    rows = normed.shape[0]
    copies[1].wait()
    logits = jnp.dot(normed, wg_ref[...], preferred_element_type=F32) + bias_ref[...]
    gates = jnp.minimum(logits, 0.0) - jnp.log1p(jnp.exp(-jnp.abs(logits)))
    lane = lane_index((rows, LANES))
    run = jnp.zeros((rows, LANES), F32)
    for h in range(heads):
        run = jnp.where(lane == h, gates[:, h : h + 1], run)
    row = row_index((rows, LANES))
    step = 1
    while step < rows:
        run = run + jnp.where(row >= step, pltpu.roll(run, step, 0), 0.0)
        step *= 2
    run_ref[...] = run
    packed = pack_lanes(run, heads).astype(BF16)
    copies[2].wait()
    new_ref[0:rows, :] = jnp.dot(normed, wk_ref[...], preferred_element_type=F32).astype(BF16)
    copies[3].wait()
    new_ref[rows : 2 * rows, :] = jnp.dot(
        normed, wv_ref[...], preferred_element_type=F32
    ).astype(BF16)
    copies[4].wait()
    queries = jnp.dot(normed, wq_ref[...], preferred_element_type=F32).astype(BF16)
    width = queries.shape[1]
    for slot in range(share_ref.shape[0]):
        share_ref[slot, :, 0:width] = queries
        share_ref[slot, :, width:] = packed


def piece_projections(tokens, gain, wq, wk, wv, wg, bias, near):
    rows, model = tokens.shape
    heads = bias.shape[0]
    width, head_dim = wq.shape[1], wk.shape[1]
    hbm = pl.BlockSpec(memory_space=pl.ANY)
    vmem = pl.BlockSpec(memory_space=pltpu.VMEM)
    return pl.pallas_call(
        functools.partial(proj_kernel, heads),
        out_shape=(
            jax.ShapeDtypeStruct((near, rows, width + LANES), BF16),
            jax.ShapeDtypeStruct((2 * rows, head_dim), BF16),
            jax.ShapeDtypeStruct((rows, LANES), F32),
        ),
        in_specs=[hbm, vmem, hbm, hbm, hbm, hbm, vmem],
        out_specs=(vmem, vmem, vmem),
        scratch_shapes=[
            pltpu.VMEM((rows, model), BF16),
            pltpu.VMEM((model, width), BF16),
            pltpu.VMEM((model, head_dim), BF16),
            pltpu.VMEM((model, head_dim), BF16),
            pltpu.VMEM((model, heads), BF16),
            pltpu.SemaphoreType.DMA((5,)),
        ],
        name="piece_proj",
    )(tokens, gain.reshape(1, model), wq, wk, wv, wg, bias.reshape(1, heads))


def pack_kernel(heads, pk_hbm, pv_hbm, gate_ref, out_ref, parts_ref, sems):
    count = pk_hbm.shape[0]
    copies = []
    for n, src in enumerate((pk_hbm, pv_hbm)):
        copy = pltpu.make_async_copy(src, out_ref.at[pl.ds(n * count, count)], sems.at[n])
        copy.start()
        copies.append(copy)
    halves = count // LANES
    block = heads * halves
    parts_ref[...] = jnp.zeros_like(parts_ref)
    for n, part in enumerate(three_parts(gate_ref[...])):
        for half in range(halves):
            at = n * block + half * heads
            parts_ref[at : at + heads, :] = part[:, half * LANES : (half + 1) * LANES]
    out_ref[2 * count :, :] = parts_ref[...].astype(BF16)
    for copy in copies:
        copy.wait()


def packed_past(past_keys, past_values, past_gate):
    count, head_dim = past_keys.shape
    heads = past_gate.shape[0]
    gate_rows = -(-3 * heads * (count // LANES) // 16) * 16
    hbm = pl.BlockSpec(memory_space=pl.ANY)
    vmem = pl.BlockSpec(memory_space=pltpu.VMEM)
    return pl.pallas_call(
        functools.partial(pack_kernel, heads),
        out_shape=jax.ShapeDtypeStruct((2 * count + gate_rows, head_dim), BF16),
        in_specs=[hbm, hbm, vmem],
        out_specs=vmem,
        scratch_shapes=[pltpu.VMEM((gate_rows, LANES), F32), pltpu.SemaphoreType.DMA((2,))],
        name="pack_past",
    )(past_keys, past_values, past_gate)


def run_kernel(heads, place_ref, shared_ref, new_ref, run_ref, out_ref):
    near, rows = shared_ref.shape[0], shared_ref.shape[1]
    width = shared_ref.shape[2] - LANES
    mine = place_ref[1]
    before = jnp.zeros((1, LANES), F32)
    total = jnp.zeros((1, LANES), F32)
    for i in range(near):
        block = shared_ref[i, :, width:].astype(F32)[rows - 1 : rows, :]
        before = before + jnp.where(i < mine, block, 0.0)
        total = total + block
    pair = jnp.concatenate([before, total, jnp.zeros((6, LANES), F32)], axis=0)
    pair = unpack_lanes(pair, heads)
    run = run_ref[...] + pair[0:1, :]
    packed = pack_lanes(run, heads)
    sums = pltpu.roll(pack_lanes(pair, heads), 16, 1)[1:2, :]
    packed = jnp.where(lane_index(packed.shape) < 16, packed, sums).astype(BF16)
    for slot in range(out_ref.shape[0]):
        out_ref[slot, 0 : 2 * rows, :] = new_ref[...]
        out_ref[slot, 2 * rows :, :] = packed


def run_payload(place, shared, new_rows, run, far, heads):
    rows = run.shape[0]
    vmem = pl.BlockSpec(memory_space=pltpu.VMEM)
    return pl.pallas_call(
        functools.partial(run_kernel, heads),
        out_shape=jax.ShapeDtypeStruct((far, 3 * rows, LANES), BF16),
        in_specs=[pl.BlockSpec(memory_space=pltpu.SMEM), vmem, vmem, vmem],
        out_specs=vmem,
        name="run_payload",
    )(place, shared, new_rows, run)


def dot_t(a, b):
    return lax.dot_general(a, b, (((1,), (1,)), ((), ())), preferred_element_type=F32)


def attend_kernel(heads, place_ref, shared_ref, new_ref, *refs):
    past_refs, out_ref = refs[:-1], refs[-1]
    far = len(past_refs)
    near, rows = shared_ref.shape[0], shared_ref.shape[1]
    head_dim = past_refs[0].shape[1]
    scale = head_dim ** (-0.5)
    width = heads * head_dim
    my_far, my_near = place_ref[0], place_ref[1]
    offset = jnp.zeros((1, LANES), F32)
    key_runs = []
    my_offset = jnp.zeros((1, LANES), F32)
    for f in range(far):
        block = unpack_lanes(new_ref[f, 2 * rows :, :].astype(F32), heads)
        key_runs.append(block + offset)
        my_offset = jnp.where(f == my_far, offset, my_offset)
        offset = offset + pltpu.roll(block, LANES - 16, 1)[0:1, :]
    new_count = far * rows
    key_run = jnp.concatenate(key_runs + [jnp.zeros((LANES - new_count, LANES), F32)], axis=0)
    key_run = jnp.transpose(key_run)
    local = unpack_lanes(
        shared_ref[:, :, width:].reshape(near * rows, LANES).astype(F32), heads
    )
    acc = my_offset
    row_runs = []
    for i in range(near):
        block = local[i * rows : (i + 1) * rows, :]
        row_runs.append(block + acc)
        acc = acc + block[rows - 1 : rows, :]
    row_run = jnp.concatenate(row_runs, axis=0)
    shape = (near * rows, LANES)
    row_place = my_far * (near * rows) + row_index(shape)
    lane = lane_index(shape)
    key_place = ((lane // rows) * near + my_near) * rows + lane % rows
    visible = (key_place <= row_place) & (lane < new_count)
    new_keys = jnp.concatenate(
        [new_ref[f, 0:rows, :] for f in range(far)]
        + [jnp.zeros((LANES - new_count, head_dim), BF16)],
        axis=0,
    )
    new_values = jnp.concatenate(
        [new_ref[f, rows : 2 * rows, :] for f in range(far)]
        + [jnp.zeros((LANES - new_count, head_dim), BF16)],
        axis=0,
    )
    count = past_rows(past_refs[0].shape[0], heads)
    halves = count // LANES
    block_rows = heads * halves
    past_gates = []
    for ref in past_refs:
        parts = ref[2 * count :, :].astype(F32)
        past_gates.append(
            parts[0:block_rows] + parts[block_rows : 2 * block_rows]
            + parts[2 * block_rows : 3 * block_rows]
        )
    lse_lanes = jnp.zeros(shape, F32)
    for h in range(heads):
        query = shared_ref[:, :, h * head_dim : (h + 1) * head_dim].reshape(near * rows, head_dim)
        scores = []
        for ref, gate in zip(past_refs, past_gates):
            row = jnp.concatenate(
                [gate[half * heads + h : half * heads + h + 1, :] for half in range(halves)], axis=1
            )
            scores.append(dot_t(query, ref[0:count, :]) * scale + row)
        fresh = dot_t(query, new_keys) * scale - key_run[h : h + 1, :]
        scores.append(jnp.where(visible, fresh, -jnp.inf))
        top = functools.reduce(
            jnp.maximum, [jnp.max(s, axis=-1, keepdims=True) for s in scores]
        )
        total = jnp.zeros((near * rows, 1), F32)
        summed = jnp.zeros((near * rows, head_dim), F32)
        for s, values in zip(scores, [ref[count : 2 * count, :] for ref in past_refs] + [new_values]):
            exponent = jnp.exp(s - top)
            total = total + jnp.sum(exponent, axis=-1, keepdims=True)
            summed = summed + jnp.dot(
                exponent.astype(BF16), values, preferred_element_type=F32
            )
        result = (summed / total).astype(BF16)
        out_ref[:, :, h * head_dim : (h + 1) * head_dim] = result.reshape(near, rows, head_dim)
        lse_lanes = jnp.where(lane == h, top + jnp.log(total), lse_lanes)
    lse_lanes = lse_lanes + jnp.where(lane < heads, row_run, 0.0)
    out_ref[:, :, width:] = (
        pack_lanes(lse_lanes, heads).astype(BF16).reshape(near, rows, LANES)
    )


def past_rows(payload_rows, heads):
    count = LANES
    while 2 * count + -(-3 * heads * (count // LANES) // 16) * 16 < payload_rows:
        count += LANES
    return count


def attend(place, shared, new_blocks, past_blocks, heads):
    vmem = pl.BlockSpec(memory_space=pltpu.VMEM)
    return pl.pallas_call(
        functools.partial(attend_kernel, heads),
        out_shape=jax.ShapeDtypeStruct(shared.shape, BF16),
        in_specs=[pl.BlockSpec(memory_space=pltpu.SMEM)] + [vmem] * (2 + len(past_blocks)),
        out_specs=vmem,
        name="attend_past",
    )(place, shared, new_blocks, *past_blocks)


def merge_kernel(heads, back_ref, out_ref):
    near, rows = back_ref.shape[0], back_ref.shape[1]
    width = back_ref.shape[2] - LANES
    head_dim = width // heads
    lse = unpack_lanes(back_ref[:, :, width:].reshape(near * rows, LANES).astype(F32), heads)
    blocks = [lse[i * rows : (i + 1) * rows, :] for i in range(near)]
    top = functools.reduce(jnp.maximum, blocks)
    weights = [jnp.exp(b - top) for b in blocks]
    total = functools.reduce(jnp.add, weights)
    for h in range(heads):
        summed = jnp.zeros((rows, head_dim), F32)
        for i in range(near):
            part = back_ref[i, :, h * head_dim : (h + 1) * head_dim].astype(F32)
            summed = summed + part * weights[i][:, h : h + 1]
        out_ref[:, h * head_dim : (h + 1) * head_dim] = (summed / total[:, h : h + 1]).astype(BF16)


def merge(back, heads):
    _, rows, wide = back.shape
    vmem = pl.BlockSpec(memory_space=pltpu.VMEM)
    return pl.pallas_call(
        functools.partial(merge_kernel, heads),
        out_shape=jax.ShapeDtypeStruct((rows, wide - LANES), BF16),
        in_specs=[vmem],
        out_specs=vmem,
        name="merge",
    )(back)


def decode(
    dec_tokens,
    norm_gain,
    query_weight,
    key_weight,
    value_weight,
    gate_weight,
    gate_bias,
    dec_keys,
    dec_values,
    dec_gate,
    dec_lengths,
):
    seq_count, new_count, model_width = dec_tokens.shape
    head_dim = dec_keys.shape[3]
    kv_local = dec_keys.shape[2]
    heads_local = gate_bias.shape[0]
    group_size = heads_local // kv_local
    score_scale = head_dim ** (-0.5)
    rows = dec_tokens.reshape(seq_count * new_count, model_width)
    normed = rms_scale(rows, norm_gain).astype(BF16)
    queries = jnp.dot(normed, query_weight, preferred_element_type=F32).astype(BF16)
    key_rows = jnp.dot(normed, key_weight, preferred_element_type=F32).astype(BF16)
    value_rows = jnp.dot(normed, value_weight, preferred_element_type=F32).astype(BF16)
    log_gates = jax.nn.log_sigmoid(
        jnp.dot(normed, gate_weight, preferred_element_type=F32) + gate_bias
    )
    dec_queries = queries.reshape(seq_count, new_count, kv_local, group_size, head_dim)
    dec_new_keys = key_rows.reshape(seq_count, new_count, kv_local, head_dim)
    dec_new_values = value_rows.reshape(seq_count, new_count, kv_local, head_dim)
    dec_run = jnp.cumsum(log_gates.reshape(seq_count, new_count, heads_local), axis=1)
    past_len = dec_keys.shape[1]
    slot_index = jnp.arange(past_len)
    last_gate = jnp.sum(
        jnp.where(slot_index[None, None, :] == (dec_lengths - 1)[:, None, None], dec_gate, 0.0),
        axis=2,
    )
    query_bias = jnp.moveaxis(dec_run.reshape(seq_count, new_count, kv_local, group_size), 1, 3)
    past_bias = last_gate.reshape(seq_count, kv_local, group_size)[..., None, None]
    dec_gate_groups = dec_gate.reshape(seq_count, kv_local, group_size, past_len)
    new_scores = (
        jnp.einsum("stkgd,sukd->skgtu", dec_queries, dec_new_keys, preferred_element_type=F32)
        * score_scale
    )
    new_scores = new_scores + query_bias[..., None] - query_bias[..., None, :]
    new_causal = jnp.arange(new_count)[None, :] <= jnp.arange(new_count)[:, None]
    new_scores = jnp.where(new_causal, new_scores, -jnp.inf)
    new_top = jnp.max(new_scores, axis=-1)
    new_exp = jnp.exp(new_scores - new_top[..., None])
    start_dec = (
        jnp.einsum(
            "skgtu,sukd->skgtd", new_exp.astype(BF16), dec_new_values, preferred_element_type=F32
        ),
        new_top,
        jnp.sum(new_exp, axis=-1),
    )
    block_scores = (
        jnp.einsum("stkgd,spkd->skgtp", dec_queries, dec_keys, preferred_element_type=F32)
        * score_scale
    )
    block_scores = (
        block_scores + query_bias[..., None] + past_bias - dec_gate_groups[:, :, :, None, :]
    )
    live_mask = jnp.arange(past_len)[None, :] < dec_lengths[:, None]
    block_scores = jnp.where(live_mask[:, None, None, None, :], block_scores, -jnp.inf)
    row_top = jnp.maximum(start_dec[1], jnp.max(block_scores, axis=-1))
    block_exp = jnp.exp(block_scores - row_top[..., None])
    rescale = jnp.exp(start_dec[1] - row_top)
    summed = start_dec[0] * rescale[..., None] + jnp.einsum(
        "skgtp,spkd->skgtd", block_exp.astype(BF16), dec_values, preferred_element_type=F32
    )
    dec_attention = summed / (start_dec[2] * rescale + jnp.sum(block_exp, axis=-1))[..., None]
    return (
        jnp.transpose(dec_attention, (0, 3, 1, 2, 4))
        .reshape(seq_count * new_count, heads_local * head_dim)
        .astype(BF16)
    )


def swapped(x):
    return lax.ppermute(x, "tp", [(0, 1), (1, 0)])


def finish(partial, out_gain):
    mixed = partial.astype(F32) + swapped(partial).astype(F32)
    return rms_scale(mixed, out_gain).astype(BF16)


def body(
    piece_tokens,
    dec_tokens,
    norm_gain,
    query_weight,
    key_weight,
    value_weight,
    gate_weight,
    gate_bias,
    out_weight,
    out_gain,
    past_keys,
    past_values,
    past_gate,
    dec_keys,
    dec_values,
    dec_gate,
    dec_lengths,
):
    heads = gate_bias.shape[0]
    far = lax.axis_size("zh")
    near = lax.axis_size(NEAR)
    place = jnp.stack([lax.axis_index("zh"), lax.axis_index(NEAR)]).astype(jnp.int32)
    my_far = lax.axis_index("zh")
    count, _, head_dim = past_keys.shape

    shares, new_rows, run = piece_projections(
        piece_tokens, norm_gain, query_weight, key_weight, value_weight, gate_weight, gate_bias, near
    )
    past_mine = packed_past(
        past_keys.reshape(count, head_dim), past_values.reshape(count, head_dim), past_gate
    )
    shared = lax.all_to_all(shares, NEAR, split_axis=0, concat_axis=0, tiled=True)
    past_blocks = [past_mine]
    for step in range(1, far):
        past_blocks.append(
            lax.ppermute(past_mine, "zh", [(k, (k + step) % far) for k in range(far)])
        )
    new_blocks = lax.all_to_all(
        run_payload(place, shared, new_rows, run, far, heads),
        "zh",
        split_axis=0,
        concat_axis=0,
        tiled=True,
    )
    partials = attend(place, shared, new_blocks, past_blocks, heads)
    back = lax.all_to_all(partials, NEAR, split_axis=0, concat_axis=0, tiled=True)
    piece_attention = merge(back, heads)
    piece_partial = jnp.dot(piece_attention, out_weight, preferred_element_type=F32).astype(BF16)

    dec_attention = decode(
        dec_tokens,
        norm_gain,
        query_weight,
        key_weight,
        value_weight,
        gate_weight,
        gate_bias,
        dec_keys,
        dec_values,
        dec_gate,
        dec_lengths,
    )
    dec_partial = jnp.dot(dec_attention, out_weight, preferred_element_type=F32).astype(BF16)
    dec_rows = finish(dec_partial, out_gain)
    piece_rows = finish(piece_partial, out_gain)
    return piece_rows, dec_rows.reshape(dec_tokens.shape)


def solution(mesh):
    finer = Mesh(
        mesh.devices.reshape(mesh.shape["dp"], 4, 2, 8, mesh.shape["tp"]),
        ("dp", "zh", "zl", "y", "tp"),
    )
    in_specs = (
        P(DP_KV, None),
        P(DP_KV, None, None),
        P(),
        P(None, "tp"),
        P(None, "tp"),
        P(None, "tp"),
        P(None, "tp"),
        P("tp"),
        P("tp", None),
        P(),
        P(DP_KV, "tp", None),
        P(DP_KV, "tp", None),
        P("tp", DP_KV),
        P(DP_KV, None, "tp", None),
        P(DP_KV, None, "tp", None),
        P(DP_KV, "tp", None),
        P(DP_KV),
    )
    out_specs = (P(DP_KV, None), P(DP_KV, None, None))
    return jax.shard_map(body, mesh=finer, in_specs=in_specs, out_specs=out_specs, check_vma=False)
```

```python
import functools

import jax
import jax.numpy as jnp
from jax import lax
from jax.experimental import pallas as pl
from jax.experimental.pallas import tpu as pltpu
from jax.sharding import Mesh
from jax.sharding import PartitionSpec as P

PART = ("z", "y", "tp")
DP_KV = ("dp", "z", "y")
FAR = 4
EPS = 1e-06
LANES = 128
F32 = jnp.float32
BF16 = jnp.bfloat16
ROOM = 20 * 1024 * 1024


def rms_scale(source, scale_gain):
    widened = source.astype(F32)
    return (
        widened * lax.rsqrt(jnp.mean(widened * widened, axis=-1, keepdims=True) + EPS) * scale_gain
    )


def three_parts(x):
    high = x.astype(BF16).astype(F32)
    rest = x - high
    middle = rest.astype(BF16).astype(F32)
    low = (rest - middle).astype(BF16).astype(F32)
    return high, middle, low


def lane_index(shape):
    return lax.broadcasted_iota(jnp.int32, shape, len(shape) - 1)


def row_index(shape):
    return lax.broadcasted_iota(jnp.int32, shape, 0)


def pack_lanes(x, heads):
    high, middle, low = three_parts(x)
    lane = lane_index(x.shape)
    middle = pltpu.roll(middle, heads, 1)
    low = pltpu.roll(low, 2 * heads, 1)
    return jnp.where(
        lane < heads,
        high,
        jnp.where(lane < 2 * heads, middle, jnp.where(lane < 3 * heads, low, 0.0)),
    )


def unpack_lanes(x, heads):
    return x + pltpu.roll(x, LANES - heads, 1) + pltpu.roll(x, LANES - 2 * heads, 1)


def proj_kernel(
    heads,
    tok_hbm,
    gain_ref,
    wq_hbm,
    wk_hbm,
    wv_hbm,
    wg_ref,
    bias_ref,
    share_ref,
    new_ref,
    tok_ref,
    wq_ref,
    wk_ref,
    wv_ref,
    sems,
):
    model, width = wq_ref.shape
    pieces = sems.shape[0] - 3
    depth = model // pieces
    moves = [(tok_hbm, tok_ref)]
    moves += [
        (wq_hbm.at[pl.ds(n * depth, depth)], wq_ref.at[pl.ds(n * depth, depth)])
        for n in range(pieces)
    ]
    moves += [(wk_hbm, wk_ref), (wv_hbm, wv_ref)]
    copies = [pltpu.make_async_copy(src, dst, sems.at[n]) for n, (src, dst) in enumerate(moves)]
    for copy in copies:
        copy.start()
    copies[0].wait()
    normed = rms_scale(tok_ref[...], gain_ref[...]).astype(BF16)
    rows = normed.shape[0]
    logits = dot_t(normed, wg_ref[...]) + bias_ref[...]
    gates = jnp.minimum(logits, 0.0) - jnp.log1p(jnp.exp(-jnp.abs(logits)))
    lane = lane_index((rows, LANES))
    run = jnp.zeros((rows, LANES), F32)
    for h in range(heads):
        run = jnp.where(lane == h, gates[:, h : h + 1], run)
    row = row_index((rows, LANES))
    step = 1
    while step < rows:
        run = run + jnp.where(row >= step, pltpu.roll(run, step, 0), 0.0)
        step *= 2
    packed = pack_lanes(run, heads).astype(BF16)
    queries = jnp.zeros((rows, width), F32)
    for n in range(pieces):
        copies[1 + n].wait()
        queries = queries + jnp.dot(
            normed[:, n * depth : (n + 1) * depth],
            wq_ref[n * depth : (n + 1) * depth, :],
            preferred_element_type=F32,
        )
    queries = queries.astype(BF16)
    for slot in range(share_ref.shape[0]):
        share_ref[slot, :, 0:width] = queries
        share_ref[slot, :, width:] = packed
    copies[1 + pieces].wait()
    new_ref[0:rows, :] = jnp.dot(normed, wk_ref[...], preferred_element_type=F32).astype(BF16)
    copies[2 + pieces].wait()
    new_ref[rows : 2 * rows, :] = jnp.dot(
        normed, wv_ref[...], preferred_element_type=F32
    ).astype(BF16)
    new_ref[2 * rows :, :] = packed


def piece_projections(tokens, gain, wq, wk, wv, wg, bias, near):
    rows, model = tokens.shape
    heads = bias.shape[0]
    width, head_dim = wq.shape[1], wk.shape[1]
    hbm = pl.BlockSpec(memory_space=pl.ANY)
    vmem = pl.BlockSpec(memory_space=pltpu.VMEM)
    return pl.pallas_call(
        functools.partial(proj_kernel, heads),
        out_shape=(
            jax.ShapeDtypeStruct((near, rows, width + LANES), BF16),
            jax.ShapeDtypeStruct((3 * rows, head_dim), BF16),
        ),
        in_specs=[hbm, vmem, hbm, hbm, hbm, vmem, vmem],
        out_specs=(vmem, vmem),
        scratch_shapes=[
            pltpu.VMEM((rows, model), BF16),
            pltpu.VMEM((model, width), BF16),
            pltpu.VMEM((model, head_dim), BF16),
            pltpu.VMEM((model, head_dim), BF16),
            pltpu.SemaphoreType.DMA((7,)),
        ],
        cost_estimate=cost(3.0, 3 << 20),
        name="piece_proj",
    )(
        tokens,
        gain.reshape(1, model),
        wq,
        wk,
        wv,
        wg.T,
        bias.reshape(1, heads),
    )


def pack_kernel(heads, pk_hbm, pv_hbm, gate_ref, past_ref, parts_ref, sems):
    count = pk_hbm.shape[0]
    moves = [(pk_hbm, past_ref.at[pl.ds(0, count)]), (pv_hbm, past_ref.at[pl.ds(count, count)])]
    copies = [pltpu.make_async_copy(src, dst, sems.at[n]) for n, (src, dst) in enumerate(moves)]
    for copy in copies:
        copy.start()
    halves = count // LANES
    block = heads * halves
    parts_ref[...] = jnp.zeros_like(parts_ref)
    for n, part in enumerate(three_parts(gate_ref[...])):
        for half in range(halves):
            at = n * block + half * heads
            parts_ref[at : at + heads, :] = part[:, half * LANES : (half + 1) * LANES]
    past_ref[2 * count :, :] = parts_ref[...].astype(BF16)
    for copy in copies:
        copy.wait()


def packed_past(past_keys, past_values, past_gate):
    count, head_dim = past_keys.shape
    heads = past_gate.shape[0]
    gate_rows = -(-3 * heads * (count // LANES) // 16) * 16
    hbm = pl.BlockSpec(memory_space=pl.ANY)
    vmem = pl.BlockSpec(memory_space=pltpu.VMEM)
    return pl.pallas_call(
        functools.partial(pack_kernel, heads),
        out_shape=jax.ShapeDtypeStruct((2 * count + gate_rows, head_dim), BF16),
        in_specs=[hbm, hbm, vmem],
        out_specs=vmem,
        scratch_shapes=[pltpu.VMEM((gate_rows, LANES), F32), pltpu.SemaphoreType.DMA((2,))],
        compiler_params=room(),
        cost_estimate=cost(2.0, 1 << 18),
        name="pack_past",
    )(past_keys, past_values, past_gate)


def room():
    return pltpu.CompilerParams(vmem_limit_bytes=ROOM)


def cost(micros, moved):
    return pl.CostEstimate(
        flops=int(micros * 15e6), bytes_accessed=int(moved), transcendentals=0
    )


def run_kernel(shared_ref, new_ref, past_ref, out_ref):
    near, rows = shared_ref.shape[0], shared_ref.shape[1]
    width = shared_ref.shape[2] - LANES
    totals = jnp.concatenate(
        [shared_ref[i, :, width:].astype(F32)[rows - 1 : rows, :] for i in range(near)], axis=0
    )
    run = new_ref[2 * rows :, :].astype(F32)
    run = jnp.where(lane_index(run.shape) < 16, run, pltpu.roll(totals, 16, 1)).astype(BF16)
    for slot in range(out_ref.shape[0]):
        out_ref[slot, 0 : 2 * rows, :] = new_ref[0 : 2 * rows, :]
        out_ref[slot, 2 * rows : 3 * rows, :] = run
        out_ref[slot, 3 * rows :, :] = past_ref[...]


def run_payload(shared, new_rows, past, far):
    near, rows, _ = shared.shape
    assert near == rows
    vmem = pl.BlockSpec(memory_space=pltpu.VMEM)
    return pl.pallas_call(
        run_kernel,
        out_shape=jax.ShapeDtypeStruct((far, 3 * rows + past.shape[0], LANES), BF16),
        in_specs=[vmem, vmem, vmem],
        out_specs=vmem,
        compiler_params=room(),
        cost_estimate=cost(1.0, 1 << 18),
        name="run_payload",
    )(shared, new_rows, past)


def dot_t(a, b):
    return lax.dot_general(a, b, (((1,), (1,)), ((), ())), preferred_element_type=F32)


def past_count(payload_rows, heads):
    count = LANES
    while 2 * count + -(-3 * heads * (count // LANES) // 16) * 16 < payload_rows:
        count += LANES
    return count


def attend_kernel(heads, sizes, place_ref, shared_ref, new_ref, out_ref):
    near, rows = shared_ref.shape[0], shared_ref.shape[1]
    far, head_dim = new_ref.shape[0], new_ref.shape[2]
    scale = head_dim ** (-0.5)
    width = heads * head_dim
    my_far, my_near = place_ref[0], place_ref[1]
    across, core = sizes[1] // far, place_ref[2]

    def block_place(block, alike):
        by_z = block * near + alike
        by_y = (alike // across) * sizes[1] + block * across + alike % across
        return jnp.where(core == 0, by_z, by_y)

    folded = [
        unpack_lanes(new_ref[f, 2 * rows : 3 * rows, :].astype(F32), heads) for f in range(far)
    ]
    totals = pltpu.roll(jnp.concatenate(folded, axis=0), LANES - 16, 1)
    shape = (8 + near, far * near)
    row = row_index(shape)
    wanted = jnp.where(row < 8, block_place(row, my_near), block_place(my_far, row - 8))
    source = lane_index(shape)
    earlier = (block_place(source // near, source % near) < wanted).astype(F32)
    before = jnp.dot(
        earlier, totals, preferred_element_type=F32, precision=lax.Precision.HIGHEST
    )
    new_count = far * rows
    key_run = jnp.concatenate(
        [folded[f] + before[f : f + 1, :] for f in range(far)]
        + [jnp.zeros((LANES - new_count, LANES), F32)],
        axis=0,
    )
    key_run = jnp.transpose(key_run)
    local = unpack_lanes(
        shared_ref[:, :, width:].reshape(near * rows, LANES).astype(F32), heads
    )
    row_run = jnp.concatenate(
        [local[i * rows : (i + 1) * rows, :] + before[8 + i : 9 + i, :] for i in range(near)],
        axis=0,
    )
    shape = (near * rows, LANES)
    row = row_index(shape)
    row_place = block_place(my_far, row // rows) * rows + row % rows
    lane = lane_index(shape)
    key_place = block_place(lane // rows, my_near) * rows + lane % rows
    visible = (key_place <= row_place) & (lane < new_count)
    new_keys = jnp.concatenate(
        [new_ref[f, 0:rows, :] for f in range(far)]
        + [jnp.zeros((LANES - new_count, head_dim), BF16)],
        axis=0,
    )
    new_values = jnp.concatenate(
        [new_ref[f, rows : 2 * rows, :] for f in range(far)]
        + [jnp.zeros((LANES - new_count, head_dim), BF16)],
        axis=0,
    )
    first = 3 * rows
    count = past_count(new_ref.shape[1] - first, heads)
    halves = count // LANES
    block = heads * halves
    gates = []
    for f in range(far):
        parts = new_ref[f, first + 2 * count :, :].astype(F32)
        gates.append(parts[0:block] + parts[block : 2 * block] + parts[2 * block : 3 * block])
    lse_lanes = jnp.zeros(shape, F32)
    for h in range(heads):
        query = shared_ref[:, :, h * head_dim : (h + 1) * head_dim].reshape(near * rows, head_dim)
        scores = []
        for f in range(far):
            row = jnp.concatenate(
                [gates[f][half * heads + h : half * heads + h + 1, :] for half in range(halves)],
                axis=1,
            )
            scores.append(dot_t(query, new_ref[f, first : first + count, :]) * scale + row)
        fresh = dot_t(query, new_keys) * scale - key_run[h : h + 1, :]
        fresh = jnp.where(visible, fresh, -jnp.inf)
        top = jnp.maximum(
            jnp.max(functools.reduce(jnp.maximum, scores), axis=-1, keepdims=True),
            jnp.max(fresh, axis=-1, keepdims=True),
        )
        fresh = jnp.exp(fresh - top)
        summed = jnp.dot(fresh.astype(BF16), new_values, preferred_element_type=F32)
        wide = jnp.zeros(scores[0].shape, F32)
        for f in range(far):
            exponent = jnp.exp(scores[f] - top)
            wide = wide + exponent
            summed = summed + jnp.dot(
                exponent.astype(BF16),
                new_ref[f, first + count : first + 2 * count, :],
                preferred_element_type=F32,
            )
        total = jnp.sum(wide, axis=-1, keepdims=True) + jnp.sum(fresh, axis=-1, keepdims=True)
        result = (summed * (1.0 / total)).astype(BF16)
        out_ref[:, :, h * head_dim : (h + 1) * head_dim] = result.reshape(near, rows, head_dim)
        lse_lanes = jnp.where(lane == h, top + jnp.log(total), lse_lanes)
    lse_lanes = lse_lanes + jnp.where(lane < heads, row_run, 0.0)
    out_ref[:, :, width:] = (
        pack_lanes(lse_lanes, heads).astype(BF16).reshape(near, rows, LANES)
    )


def attend(place, shared, new_blocks, heads, sizes):
    vmem = pl.BlockSpec(memory_space=pltpu.VMEM)
    return pl.pallas_call(
        functools.partial(attend_kernel, heads, sizes),
        out_shape=jax.ShapeDtypeStruct(shared.shape, BF16),
        in_specs=[pl.BlockSpec(memory_space=pltpu.SMEM), vmem, vmem],
        out_specs=vmem,
        compiler_params=room(),
        cost_estimate=cost(4.0, 1 << 20),
        name="attend",
    )(place, shared, new_blocks)


def merge_kernel(heads, back_ref, wo_ref, out_ref):
    near, rows = back_ref.shape[0], back_ref.shape[1]
    width = back_ref.shape[2] - LANES
    head_dim = width // heads
    lse = unpack_lanes(back_ref[:, :, width:].reshape(near * rows, LANES).astype(F32), heads)
    blocks = [lse[i * rows : (i + 1) * rows, :] for i in range(near)]
    top = functools.reduce(jnp.maximum, blocks)
    weights = [jnp.exp(b - top) for b in blocks]
    inverse = 1.0 / functools.reduce(jnp.add, weights)
    weights = [w * inverse for w in weights]
    merged = []
    for h in range(heads):
        summed = jnp.zeros((rows, head_dim), F32)
        for i in range(near):
            part = back_ref[i, :, h * head_dim : (h + 1) * head_dim].astype(F32)
            summed = summed + part * weights[i][:, h : h + 1]
        merged.append(summed.astype(BF16))
    attention = jnp.concatenate(merged, axis=1)
    out_ref[...] = jnp.dot(attention, wo_ref[...], preferred_element_type=F32).astype(BF16)


def merge(back, out_weight, heads):
    _, rows, _ = back.shape
    vmem = pl.BlockSpec(memory_space=pltpu.VMEM)
    return pl.pallas_call(
        functools.partial(merge_kernel, heads),
        out_shape=jax.ShapeDtypeStruct((rows, out_weight.shape[1]), BF16),
        in_specs=[vmem, vmem],
        out_specs=vmem,
        compiler_params=room(),
        cost_estimate=cost(2.0, 2 << 20),
        name="merge",
    )(back, out_weight)


def final_kernel(one_ref, two_ref, gain_ref, out_ref):
    mixed = one_ref[...].astype(F32) + two_ref[...].astype(F32)
    out_ref[...] = rms_scale(mixed, gain_ref[...]).astype(BF16)


def final(one, two, gain):
    vmem = pl.BlockSpec(memory_space=pltpu.VMEM)
    return pl.pallas_call(
        final_kernel,
        out_shape=jax.ShapeDtypeStruct(one.shape, BF16),
        in_specs=[vmem] * 3,
        out_specs=vmem,
        compiler_params=room(),
        cost_estimate=cost(0.5, 1 << 17),
        name="final",
    )(one, two, gain.reshape(1, -1))


def dec_kernel(
    lengths_ref,
    tok_hbm,
    gain_ref,
    wq_hbm,
    wk_hbm,
    wv_hbm,
    wg_ref,
    bias_ref,
    keys_hbm,
    values_hbm,
    gate_hbm,
    wo_hbm,
    out_ref,
    wo_ref,
    tok_ref,
    wq_ref,
    wk_ref,
    wv_ref,
    keys_ref,
    values_ref,
    gate_ref,
    rows_ref,
    query_ref,
    run_ref,
    bias_rows_ref,
    score_ref,
    result_ref,
    sems,
):
    seqs, new, _ = tok_ref.shape
    width = wq_ref.shape[1]
    past, head_dim = keys_ref.shape[1], keys_ref.shape[2]
    heads = width // head_dim
    scale = head_dim ** (-0.5)
    each = heads * new
    total_rows = seqs * each
    moves = (
        (tok_hbm, tok_ref),
        (wq_hbm, wq_ref),
        (wk_hbm, wk_ref),
        (wv_hbm, wv_ref),
        (gate_hbm, gate_ref),
        (keys_hbm, keys_ref),
        (values_hbm, values_ref),
        (wo_hbm, wo_ref),
    )
    copies = [pltpu.make_async_copy(src, dst, sems.at[n]) for n, (src, dst) in enumerate(moves)]
    for copy in copies:
        copy.start()
    copies[0].wait()
    for s in range(seqs):
        rows_ref[s * new : (s + 1) * new, :] = tok_ref[s].astype(F32)
    normed = rms_scale(rows_ref[...], gain_ref[...]).astype(BF16)
    rows = seqs * new
    logits = dot_t(normed, wg_ref[...]) + bias_ref[...]
    gates = jnp.minimum(logits, 0.0) - jnp.log1p(jnp.exp(-jnp.abs(logits)))
    lane = lane_index((rows, LANES))
    row = row_index((rows, LANES))
    run = jnp.zeros((rows, LANES), F32)
    for h in range(heads):
        run = jnp.where(lane == h, gates[:, h : h + 1], run)
    step = 1
    while step < new:
        run = run + jnp.where(row % new >= step, pltpu.roll(run, step, 0), 0.0)
        step *= 2
    copies[1].wait()
    queries = jnp.dot(normed, wq_ref[...], preferred_element_type=F32)
    copies[2].wait()
    pad = jnp.zeros((LANES - rows, head_dim), BF16)
    new_keys = jnp.dot(normed, wk_ref[...], preferred_element_type=F32).astype(BF16)
    copies[3].wait()
    new_values = jnp.dot(normed, wv_ref[...], preferred_element_type=F32).astype(BF16)
    new_keys = jnp.concatenate([new_keys, pad], axis=0)
    new_values = jnp.concatenate([new_values, pad], axis=0)
    copies[4].wait()
    for s in range(seqs):
        for h in range(heads):
            at = s * each + h * new
            query_ref[at : at + new, :] = queries[
                s * new : (s + 1) * new, h * head_dim : (h + 1) * head_dim
            ]
            run_ref[at : at + new, :] = run[s * new : (s + 1) * new, :]
            bias_rows_ref[at : at + new, :] = jnp.broadcast_to(
                gate_ref[s, h : h + 1, :], (new, past)
            )
    query = query_ref[...].astype(BF16)
    copies[5].wait()
    for s in range(seqs):
        score_ref[s * each : (s + 1) * each, :] = dot_t(
            query[s * each : (s + 1) * each, :], keys_ref[s]
        )
    lane = lane_index((total_rows, LANES))
    row = row_index((total_rows, LANES))
    head = (row // new) % heads
    row_run = jnp.sum(jnp.where(lane == head, run_ref[...], 0.0), axis=-1, keepdims=True)
    length = jnp.zeros((total_rows, LANES), jnp.int32)
    for s in range(seqs):
        length = jnp.where(row // each == s, lengths_ref[s], length)
    length = length[:, 0:1]
    slot = lane_index((total_rows, past))
    gate = bias_rows_ref[...]
    last = jnp.sum(jnp.where(slot == length - 1, gate, 0.0), axis=-1, keepdims=True)
    scores = score_ref[...] * scale + (last - gate) + row_run
    scores = jnp.where(slot < length, scores, -jnp.inf)
    by_key = jnp.transpose(
        jnp.concatenate([run, jnp.zeros((LANES - rows, LANES), F32)], axis=0)
    )
    key_run = jnp.zeros((total_rows, LANES), F32)
    for h in range(heads):
        key_run = jnp.where(head == h, by_key[h : h + 1, :], key_run)
    fresh = dot_t(query, new_keys) * scale + row_run - key_run
    visible = (lane // new == row // each) & (lane % new <= row % new)
    fresh = jnp.where(visible, fresh, -jnp.inf)
    top = jnp.maximum(
        jnp.max(scores, axis=-1, keepdims=True), jnp.max(fresh, axis=-1, keepdims=True)
    )
    weights = jnp.exp(scores - top)
    fresh = jnp.exp(fresh - top)
    total = jnp.sum(weights, axis=-1, keepdims=True) + jnp.sum(fresh, axis=-1, keepdims=True)
    inverse = 1.0 / total
    weights = weights.astype(BF16)
    summed = jnp.dot(fresh.astype(BF16), new_values, preferred_element_type=F32)
    copies[6].wait()
    for s in range(seqs):
        part = slice(s * each, (s + 1) * each)
        attention = summed[part, :] + jnp.dot(
            weights[part, :], values_ref[s], preferred_element_type=F32
        )
        attention = attention * inverse[part, :]
        for h in range(heads):
            result_ref[s * new : (s + 1) * new, h * head_dim : (h + 1) * head_dim] = attention[
                h * new : (h + 1) * new, :
            ]
    copies[7].wait()
    out_ref[...] = jnp.dot(
        result_ref[...].astype(BF16), wo_ref[...], preferred_element_type=F32
    ).astype(BF16)


def decode(tokens, gain, wq, wk, wv, wg, bias, keys, values, gate, lengths, wo):
    seqs, new, model = tokens.shape
    heads = bias.shape[0]
    width, head_dim = wq.shape[1], wk.shape[1]
    past = keys.shape[1]
    each = heads * new
    hbm = pl.BlockSpec(memory_space=pl.ANY)
    vmem = pl.BlockSpec(memory_space=pltpu.VMEM)
    return pl.pallas_call(
        dec_kernel,
        out_shape=jax.ShapeDtypeStruct((seqs * new, wo.shape[1]), BF16),
        in_specs=[
            pl.BlockSpec(memory_space=pltpu.SMEM),
            hbm,
            vmem,
            hbm,
            hbm,
            hbm,
            vmem,
            vmem,
            hbm,
            hbm,
            hbm,
            hbm,
        ],
        out_specs=vmem,
        scratch_shapes=[
            pltpu.VMEM(wo.shape, BF16),
            pltpu.VMEM((seqs, new, model), BF16),
            pltpu.VMEM((model, width), BF16),
            pltpu.VMEM((model, head_dim), BF16),
            pltpu.VMEM((model, head_dim), BF16),
            pltpu.VMEM((seqs, past, head_dim), BF16),
            pltpu.VMEM((seqs, past, head_dim), BF16),
            pltpu.VMEM((seqs, heads, past), F32),
            pltpu.VMEM((seqs * new, model), F32),
            pltpu.VMEM((seqs * each, head_dim), F32),
            pltpu.VMEM((seqs * each, LANES), F32),
            pltpu.VMEM((seqs * each, past), F32),
            pltpu.VMEM((seqs * each, past), F32),
            pltpu.VMEM((seqs * new, width), F32),
            pltpu.SemaphoreType.DMA((8,)),
        ],
        cost_estimate=cost(6.0, 8 << 20),
        name="decode",
    )(
        lengths,
        tokens,
        gain.reshape(1, model),
        wq,
        wk,
        wv,
        wg.T,
        bias.reshape(1, heads),
        keys.reshape(seqs, past, head_dim),
        values.reshape(seqs, past, head_dim),
        gate,
        wo,
    )


def groups(sizes, cores):
    far = FAR
    deep, across = sizes[0] // far, sizes[1] // far
    alike, block = {}, {}
    for z in range(sizes[0]):
        for y in range(sizes[1]):
            for core in range(cores):
                index = (z * sizes[1] + y) * cores + core
                first = core % 2 == 0
                alike.setdefault((core, z // deep if first else y // across), []).append(index)
                block.setdefault(
                    (core, z % deep if first else y % across, y if first else z), []
                ).append(index)
    return far, list(alike.values()), list(block.values())


def exchange(x, members):
    return lax.all_to_all(
        x, PART, split_axis=0, concat_axis=0, axis_index_groups=members, tiled=True
    )


def swapped(x):
    return lax.ppermute(x, "tp", [(0, 1), (1, 0)])


def layer(
    piece_tokens,
    dec_tokens,
    norm_gain,
    query_weight,
    key_weight,
    value_weight,
    gate_weight,
    gate_bias,
    out_weight,
    out_gain,
    past_keys,
    past_values,
    past_gate,
    dec_keys,
    dec_values,
    dec_gate,
    dec_lengths,
):
    heads = gate_bias.shape[0]
    sizes = (lax.axis_size("z"), lax.axis_size("y"))
    far, alike, block = groups(sizes, lax.axis_size("tp"))
    near = sizes[0] * sizes[1] // far
    z, y, core = (lax.axis_index(name) for name in PART)
    deep, across = sizes[0] // far, sizes[1] // far
    place = jnp.stack(
        [
            jnp.where(core == 0, z // deep, y // across),
            jnp.where(core == 0, (z % deep) * sizes[1] + y, z * across + y % across),
            core,
        ]
    ).astype(jnp.int32)
    count, _, head_dim = past_keys.shape

    shares, new_rows = piece_projections(
        piece_tokens, norm_gain, query_weight, key_weight, value_weight, gate_weight, gate_bias, near
    )
    shared = exchange(shares, alike)
    past_gate, shared = lax.optimization_barrier((past_gate, shared))
    past = packed_past(
        past_keys.reshape(count, head_dim), past_values.reshape(count, head_dim), past_gate
    )
    payload = run_payload(shared, new_rows, past, far)
    new_blocks = exchange(payload, block)
    partials = attend(place, shared, new_blocks, heads, sizes)
    back = exchange(partials, alike)
    dec_partial = decode(
        dec_tokens,
        norm_gain,
        query_weight,
        key_weight,
        value_weight,
        gate_weight,
        gate_bias,
        dec_keys,
        dec_values,
        dec_gate,
        dec_lengths,
        out_weight,
    )
    dec_rows = final(dec_partial, swapped(dec_partial), out_gain)
    piece_partial = merge(back, out_weight, heads)
    piece_rows = final(piece_partial, swapped(piece_partial), out_gain)
    return piece_rows, dec_rows.reshape(dec_tokens.shape)


def solution(mesh):
    finer = Mesh(
        mesh.devices.reshape(mesh.shape["dp"], 8, 8, mesh.shape["tp"]),
        ("dp", "z", "y", "tp"),
    )
    in_specs = (
        P(DP_KV, None),
        P(DP_KV, None, None),
        P(),
        P(None, "tp"),
        P(None, "tp"),
        P(None, "tp"),
        P(None, "tp"),
        P("tp"),
        P("tp", None),
        P(),
        P(DP_KV, "tp", None),
        P(DP_KV, "tp", None),
        P("tp", DP_KV),
        P(DP_KV, None, "tp", None),
        P(DP_KV, None, "tp", None),
        P(DP_KV, "tp", None),
        P(DP_KV),
    )
    out_specs = (P(DP_KV, None), P(DP_KV, None, None))
    return jax.shard_map(layer, mesh=finer, in_specs=in_specs, out_specs=out_specs, check_vma=False)
```

```python
import functools

import jax
import jax.numpy as jnp
from jax import lax
from jax.experimental import pallas as pl
from jax.experimental.pallas import tpu as pltpu
from jax.sharding import Mesh
from jax.sharding import PartitionSpec as P

PART = ("z", "y", "tp")
DP_KV = ("dp", "z", "y")
FAR = 4
EPS = 1e-06
LANES = 128
F32 = jnp.float32
BF16 = jnp.bfloat16
ROOM = 20 * 1024 * 1024


def rms_scale(source, scale_gain):
    widened = source.astype(F32)
    return (
        widened * lax.rsqrt(jnp.mean(widened * widened, axis=-1, keepdims=True) + EPS) * scale_gain
    )


def three_parts(x):
    high = x.astype(BF16).astype(F32)
    rest = x - high
    middle = rest.astype(BF16).astype(F32)
    low = (rest - middle).astype(BF16).astype(F32)
    return high, middle, low


def lane_index(shape):
    return lax.broadcasted_iota(jnp.int32, shape, len(shape) - 1)


def row_index(shape):
    return lax.broadcasted_iota(jnp.int32, shape, 0)


def pack_lanes(x, heads):
    high, middle, low = three_parts(x)
    lane = lane_index(x.shape)
    middle = pltpu.roll(middle, heads, 1)
    low = pltpu.roll(low, 2 * heads, 1)
    return jnp.where(
        lane < heads,
        high,
        jnp.where(lane < 2 * heads, middle, jnp.where(lane < 3 * heads, low, 0.0)),
    )


def unpack_lanes(x, heads):
    return x + pltpu.roll(x, LANES - heads, 1) + pltpu.roll(x, LANES - 2 * heads, 1)


def my_place(sizes, far):
    z, y, core = (lax.axis_index(name) for name in PART)
    deep, across = sizes[0] // far, sizes[1] // far
    first = core == 0
    return (
        jnp.where(first, z // deep, y // across),
        jnp.where(first, (z % deep) * sizes[1] + y, z * across + y % across),
        core,
    )


def fold_rows(x):
    half = x.shape[0] // 2
    upper, lower = x[0:half, :], x[half:, :]
    return jnp.where(lane_index(upper.shape) < 16, upper, pltpu.roll(lower, 16, 1))


def unfold_rows(x):
    return x, pltpu.roll(x, LANES - 16, 1)


def proj_kernel(
    heads, tok_hbm, gain_ref, wq_hbm, wg_ref, bias_ref, share_ref, tok_ref, wq_ref, sems
):
    model, width = wq_ref.shape
    pieces = sems.shape[0] - 1
    depth = model // pieces
    moves = [(tok_hbm, tok_ref)]
    moves += [
        (wq_hbm.at[pl.ds(n * depth, depth)], wq_ref.at[pl.ds(n * depth, depth)])
        for n in range(pieces)
    ]
    copies = [pltpu.make_async_copy(src, dst, sems.at[n]) for n, (src, dst) in enumerate(moves)]
    for copy in copies:
        copy.start()
    copies[0].wait()
    normed = rms_scale(tok_ref[...], gain_ref[...]).astype(BF16)
    rows = normed.shape[0]
    logits = dot_t(normed, wg_ref[...]) + bias_ref[...]
    gates = jnp.minimum(logits, 0.0) - jnp.log1p(jnp.exp(-jnp.abs(logits)))
    lane = lane_index((rows, LANES))
    run = jnp.zeros((rows, LANES), F32)
    for h in range(heads):
        run = jnp.where(lane == h, gates[:, h : h + 1], run)
    row = row_index((rows, LANES))
    step = 1
    while step < rows:
        run = run + jnp.where(row >= step, pltpu.roll(run, step, 0), 0.0)
        step *= 2
    packed = fold_rows(pack_lanes(run, heads)).astype(BF16)
    queries = jnp.zeros((rows, width), F32)
    for n in range(pieces):
        copies[1 + n].wait()
        queries = queries + jnp.dot(
            normed[:, n * depth : (n + 1) * depth],
            wq_ref[n * depth : (n + 1) * depth, :],
            preferred_element_type=F32,
        )
    queries = queries.astype(BF16)
    head_dim = width // heads
    for slot in range(share_ref.shape[0]):
        for h in range(heads):
            share_ref[slot, h * rows : (h + 1) * rows, :] = queries[
                :, h * head_dim : (h + 1) * head_dim
            ]
        share_ref[slot, heads * rows :, :] = packed


def piece_queries(tokens, gain, wq, wg, bias, near):
    rows, model = tokens.shape
    heads = bias.shape[0]
    width = wq.shape[1]
    hbm = pl.BlockSpec(memory_space=pl.ANY)
    vmem = pl.BlockSpec(memory_space=pltpu.VMEM)
    return pl.pallas_call(
        functools.partial(proj_kernel, heads),
        out_shape=jax.ShapeDtypeStruct(
            (near, heads * rows + rows // 2, width // heads), BF16
        ),
        in_specs=[hbm, vmem, hbm, vmem, vmem],
        out_specs=vmem,
        scratch_shapes=[
            pltpu.VMEM((rows, model), BF16),
            pltpu.VMEM((model, width), BF16),
            pltpu.SemaphoreType.DMA((5,)),
        ],
        cost_estimate=cost(3.0, 2 << 20),
        name="piece_queries",
    )(tokens, gain.reshape(1, model), wq, wg.T, bias.reshape(1, heads))


def payload_kernel(
    heads,
    sizes,
    shared_ref,
    tok_ref,
    gain_ref,
    wk_ref,
    wv_ref,
    pk_ref,
    pv_ref,
    gate_ref,
    out_ref,
    parts_ref,
):
    rows = tok_ref.shape[0]
    near = shared_ref.shape[0]
    tail = heads * rows
    count = pk_ref.shape[0]
    normed = rms_scale(tok_ref[...], gain_ref[...]).astype(BF16)
    keys = jnp.dot(normed, wk_ref[...], preferred_element_type=F32).astype(BF16)
    values = jnp.dot(normed, wv_ref[...], preferred_element_type=F32).astype(BF16)
    my_near = my_place(sizes, out_ref.shape[0])[1]
    mine = shared_ref[my_near, tail:, :].astype(F32)
    run = jnp.concatenate(unfold_rows(mine), axis=0)
    totals = jnp.concatenate(
        [shared_ref[i, tail:, :].astype(F32)[rows // 2 - 1 : rows // 2, :] for i in range(near)],
        axis=0,
    )
    run = jnp.where(lane_index(run.shape) < 16, run, totals).astype(BF16)
    halves = count // LANES
    block = heads * halves
    parts_ref[...] = jnp.zeros_like(parts_ref)
    for n, part in enumerate(three_parts(gate_ref[...])):
        for half in range(halves):
            at = n * block + half * heads
            parts_ref[at : at + heads, :] = part[:, half * LANES : (half + 1) * LANES]
    parts = parts_ref[...].astype(BF16)
    first = 3 * rows
    for slot in range(out_ref.shape[0]):
        out_ref[slot, 0:rows, :] = keys
        out_ref[slot, rows : 2 * rows, :] = values
        out_ref[slot, 2 * rows : first, :] = run
        out_ref[slot, first : first + count, :] = pk_ref[...]
        out_ref[slot, first + count : first + 2 * count, :] = pv_ref[...]
        out_ref[slot, first + 2 * count :, :] = parts


def block_payload(sizes, shared, tokens, gain, wk, wv, past_keys, past_values, past_gate, far):
    rows, model = tokens.shape
    assert shared.shape[0] == rows
    count, head_dim = past_keys.shape
    heads = past_gate.shape[0]
    gate_rows = -(-3 * heads * (count // LANES) // 16) * 16
    vmem = pl.BlockSpec(memory_space=pltpu.VMEM)
    return pl.pallas_call(
        functools.partial(payload_kernel, heads, sizes),
        out_shape=jax.ShapeDtypeStruct(
            (far, 3 * rows + 2 * count + gate_rows, head_dim), BF16
        ),
        in_specs=[vmem] * 8,
        out_specs=vmem,
        scratch_shapes=[pltpu.VMEM((gate_rows, LANES), F32)],
        compiler_params=room(),
        cost_estimate=cost(2.0, 2 << 20),
        name="block_payload",
    )(
        shared,
        tokens,
        gain.reshape(1, model),
        wk,
        wv,
        past_keys,
        past_values,
        past_gate,
    )


def room():
    return pltpu.CompilerParams(vmem_limit_bytes=ROOM)


def cost(micros, moved):
    return pl.CostEstimate(
        flops=int(micros * 15e6), bytes_accessed=int(moved), transcendentals=0
    )


def dot_t(a, b):
    return lax.dot_general(a, b, (((1,), (1,)), ((), ())), preferred_element_type=F32)


def past_count(payload_rows, heads):
    count = LANES
    while 2 * count + -(-3 * heads * (count // LANES) // 16) * 16 < payload_rows:
        count += LANES
    return count


def attend_kernel(heads, sizes, shared_ref, new_ref, out_ref):
    near, tail = shared_ref.shape[0], shared_ref.shape[1] * (2 * heads) // (2 * heads + 1)
    rows = tail // heads
    far, head_dim = new_ref.shape[0], new_ref.shape[2]
    scale = head_dim ** (-0.5)
    my_far, my_near, core = my_place(sizes, far)
    across = sizes[1] // far

    def block_place(block, alike):
        by_z = block * near + alike
        by_y = (alike // across) * sizes[1] + block * across + alike % across
        return jnp.where(core == 0, by_z, by_y)

    folded = [
        unpack_lanes(new_ref[f, 2 * rows : 3 * rows, :].astype(F32), heads) for f in range(far)
    ]
    totals = pltpu.roll(jnp.concatenate(folded, axis=0), LANES - 16, 1)
    shape = (8 + near, far * near)
    row = row_index(shape)
    wanted = jnp.where(row < 8, block_place(row, my_near), block_place(my_far, row - 8))
    source = lane_index(shape)
    earlier = (block_place(source // near, source % near) < wanted).astype(F32)
    before = jnp.dot(
        earlier, totals, preferred_element_type=F32, precision=lax.Precision.HIGHEST
    )
    new_count = far * rows
    key_run = jnp.concatenate(
        [folded[f] + before[f : f + 1, :] for f in range(far)]
        + [jnp.zeros((LANES - new_count, LANES), F32)],
        axis=0,
    )
    key_run = jnp.transpose(key_run)
    half = rows // 2
    upper, lower = (
        unpack_lanes(x, heads)
        for x in unfold_rows(shared_ref[:, tail:, :].astype(F32).reshape(near * half, LANES))
    )
    row_runs = []
    for i in range(near):
        start = before[8 + i : 9 + i, :]
        row_runs.append(upper[i * half : (i + 1) * half, :] + start)
        row_runs.append(lower[i * half : (i + 1) * half, :] + start)
    row_run = jnp.concatenate(row_runs, axis=0)
    shape = (near * rows, LANES)
    row = row_index(shape)
    row_place = block_place(my_far, row // rows) * rows + row % rows
    lane = lane_index(shape)
    key_place = block_place(lane // rows, my_near) * rows + lane % rows
    visible = (key_place <= row_place) & (lane < new_count)
    new_keys = jnp.concatenate(
        [new_ref[f, 0:rows, :] for f in range(far)]
        + [jnp.zeros((LANES - new_count, head_dim), BF16)],
        axis=0,
    )
    new_values = jnp.concatenate(
        [new_ref[f, rows : 2 * rows, :] for f in range(far)]
        + [jnp.zeros((LANES - new_count, head_dim), BF16)],
        axis=0,
    )
    first = 3 * rows
    count = past_count(new_ref.shape[1] - first, heads)
    halves = count // LANES
    block = heads * halves
    gates = []
    for f in range(far):
        parts = new_ref[f, first + 2 * count :, :].astype(F32)
        gates.append(parts[0:block] + parts[block : 2 * block] + parts[2 * block : 3 * block])
    lse_lanes = jnp.zeros(shape, F32)
    for h in range(heads):
        query = shared_ref[:, h * rows : (h + 1) * rows, :].reshape(near * rows, head_dim)
        scores = []
        for f in range(far):
            row = jnp.concatenate(
                [gates[f][half * heads + h : half * heads + h + 1, :] for half in range(halves)],
                axis=1,
            )
            scores.append(dot_t(query, new_ref[f, first : first + count, :]) * scale + row)
        fresh = dot_t(query, new_keys) * scale - key_run[h : h + 1, :]
        fresh = jnp.where(visible, fresh, -jnp.inf)
        top = jnp.maximum(
            jnp.max(functools.reduce(jnp.maximum, scores), axis=-1, keepdims=True),
            jnp.max(fresh, axis=-1, keepdims=True),
        )
        fresh = jnp.exp(fresh - top)
        summed = jnp.dot(fresh.astype(BF16), new_values, preferred_element_type=F32)
        wide = jnp.zeros(scores[0].shape, F32)
        for f in range(far):
            exponent = jnp.exp(scores[f] - top)
            wide = wide + exponent
            summed = summed + jnp.dot(
                exponent.astype(BF16),
                new_ref[f, first + count : first + 2 * count, :],
                preferred_element_type=F32,
            )
        total = jnp.sum(wide, axis=-1, keepdims=True) + jnp.sum(fresh, axis=-1, keepdims=True)
        result = (summed * (1.0 / total)).astype(BF16)
        out_ref[:, h * rows : (h + 1) * rows, :] = result.reshape(near, rows, head_dim)
        lse_lanes = jnp.where(lane == h, top + jnp.log(total), lse_lanes)
    lse_lanes = lse_lanes + jnp.where(lane < heads, row_run, 0.0)
    packed = pack_lanes(lse_lanes, heads).reshape(near, 2, half, LANES)
    folded = jnp.where(
        lane_index((near * half, LANES)) < 16,
        packed[:, 0].reshape(near * half, LANES),
        pltpu.roll(packed[:, 1].reshape(near * half, LANES), 16, 1),
    )
    out_ref[:, tail:, :] = folded.astype(BF16).reshape(near, half, LANES)


def attend(shared, new_blocks, heads, sizes):
    vmem = pl.BlockSpec(memory_space=pltpu.VMEM)
    return pl.pallas_call(
        functools.partial(attend_kernel, heads, sizes),
        out_shape=jax.ShapeDtypeStruct(shared.shape, BF16),
        in_specs=[vmem, vmem],
        out_specs=vmem,
        compiler_params=room(),
        cost_estimate=cost(4.0, 1 << 20),
        name="attend",
    )(shared, new_blocks)


def merge_kernel(heads, back_ref, wo_ref, dec_ref, out_ref):
    near, tail = back_ref.shape[0], back_ref.shape[1] * (2 * heads) // (2 * heads + 1)
    rows = tail // heads
    half = rows // 2
    head_dim = back_ref.shape[2]
    upper, lower = (
        unpack_lanes(x, heads)
        for x in unfold_rows(back_ref[:, tail:, :].astype(F32).reshape(near * half, LANES))
    )
    blocks = [
        jnp.concatenate([x[i * half : (i + 1) * half, :] for x in (upper, lower)], axis=0)
        for i in range(near)
    ]
    top = functools.reduce(jnp.maximum, blocks)
    weights = [jnp.exp(b - top) for b in blocks]
    inverse = 1.0 / functools.reduce(jnp.add, weights)
    weights = [w * inverse for w in weights]
    merged = []
    for h in range(heads):
        summed = jnp.zeros((rows, head_dim), F32)
        for i in range(near):
            part = back_ref[i, h * rows : (h + 1) * rows, :].astype(F32)
            summed = summed + part * weights[i][:, h : h + 1]
        merged.append(summed.astype(BF16))
    attention = jnp.concatenate(merged, axis=1)
    out_ref[0:rows, :] = jnp.dot(
        attention, wo_ref[...], preferred_element_type=F32
    ).astype(BF16)
    out_ref[rows:, :] = dec_ref[rows:, :]


def merge(back, out_weight, dec_partial, heads):
    vmem = pl.BlockSpec(memory_space=pltpu.VMEM)
    return pl.pallas_call(
        functools.partial(merge_kernel, heads),
        out_shape=jax.ShapeDtypeStruct(
            (dec_partial.shape[0], out_weight.shape[1]), BF16
        ),
        in_specs=[vmem, vmem, vmem],
        out_specs=vmem,
        compiler_params=room(),
        cost_estimate=cost(2.0, 2 << 20),
        name="merge",
    )(back, out_weight, dec_partial)


def final_kernel(one_ref, two_ref, gain_ref, piece_ref, dec_ref, held_ref):
    mixed = one_ref[...].astype(F32) + two_ref[...].astype(F32)
    rows = rms_scale(mixed, gain_ref[...])
    count, new = piece_ref.shape[0], dec_ref.shape[1]
    piece_ref[...] = rows[0:count, :].astype(BF16)
    held_ref[...] = rows[count:, :]
    for s in range(dec_ref.shape[0]):
        dec_ref[s] = held_ref[s * new : (s + 1) * new, :].astype(BF16)


def final(one, two, gain, piece_shape, dec_shape):
    vmem = pl.BlockSpec(memory_space=pltpu.VMEM)
    return pl.pallas_call(
        final_kernel,
        out_shape=(
            jax.ShapeDtypeStruct(piece_shape, BF16),
            jax.ShapeDtypeStruct(dec_shape, BF16),
        ),
        in_specs=[vmem] * 3,
        out_specs=(vmem, vmem),
        scratch_shapes=[pltpu.VMEM((one.shape[0] - piece_shape[0], one.shape[1]), F32)],
        compiler_params=room(),
        cost_estimate=cost(0.5, 1 << 17),
        name="final",
    )(one, two, gain.reshape(1, -1))


def dec_kernel(
    lengths_ref,
    tok_hbm,
    gain_ref,
    wq_hbm,
    wk_hbm,
    wv_hbm,
    wg_ref,
    bias_ref,
    keys_hbm,
    values_hbm,
    gate_hbm,
    wo_hbm,
    out_ref,
    wo_ref,
    tok_ref,
    wq_ref,
    wk_ref,
    wv_ref,
    keys_ref,
    values_ref,
    gate_ref,
    rows_ref,
    query_ref,
    run_ref,
    bias_rows_ref,
    score_ref,
    result_ref,
    sems,
):
    seqs, new, _ = tok_ref.shape
    width = wq_ref.shape[1]
    past, head_dim = keys_ref.shape[1], keys_ref.shape[2]
    heads = width // head_dim
    scale = head_dim ** (-0.5)
    each = heads * new
    total_rows = seqs * each
    moves = (
        (tok_hbm, tok_ref),
        (wq_hbm, wq_ref),
        (wk_hbm, wk_ref),
        (wv_hbm, wv_ref),
        (gate_hbm, gate_ref),
        (keys_hbm, keys_ref),
        (values_hbm, values_ref),
        (wo_hbm, wo_ref),
    )
    copies = [pltpu.make_async_copy(src, dst, sems.at[n]) for n, (src, dst) in enumerate(moves)]
    for copy in copies:
        copy.start()
    copies[0].wait()
    for s in range(seqs):
        rows_ref[s * new : (s + 1) * new, :] = tok_ref[s].astype(F32)
    normed = rms_scale(rows_ref[...], gain_ref[...]).astype(BF16)
    rows = seqs * new
    logits = dot_t(normed, wg_ref[...]) + bias_ref[...]
    gates = jnp.minimum(logits, 0.0) - jnp.log1p(jnp.exp(-jnp.abs(logits)))
    lane = lane_index((rows, LANES))
    row = row_index((rows, LANES))
    run = jnp.zeros((rows, LANES), F32)
    for h in range(heads):
        run = jnp.where(lane == h, gates[:, h : h + 1], run)
    step = 1
    while step < new:
        run = run + jnp.where(row % new >= step, pltpu.roll(run, step, 0), 0.0)
        step *= 2
    copies[1].wait()
    queries = jnp.dot(normed, wq_ref[...], preferred_element_type=F32)
    copies[2].wait()
    pad = jnp.zeros((LANES - rows, head_dim), BF16)
    new_keys = jnp.dot(normed, wk_ref[...], preferred_element_type=F32).astype(BF16)
    copies[3].wait()
    new_values = jnp.dot(normed, wv_ref[...], preferred_element_type=F32).astype(BF16)
    new_keys = jnp.concatenate([new_keys, pad], axis=0)
    new_values = jnp.concatenate([new_values, pad], axis=0)
    copies[4].wait()
    for s in range(seqs):
        for h in range(heads):
            at = s * each + h * new
            query_ref[at : at + new, :] = queries[
                s * new : (s + 1) * new, h * head_dim : (h + 1) * head_dim
            ]
            run_ref[at : at + new, :] = run[s * new : (s + 1) * new, :]
            bias_rows_ref[at : at + new, :] = jnp.broadcast_to(
                gate_ref[s, h : h + 1, :], (new, past)
            )
    query = query_ref[...].astype(BF16)
    copies[5].wait()
    for s in range(seqs):
        score_ref[s * each : (s + 1) * each, :] = dot_t(
            query[s * each : (s + 1) * each, :], keys_ref[s]
        )
    lane = lane_index((total_rows, LANES))
    row = row_index((total_rows, LANES))
    head = (row // new) % heads
    row_run = jnp.sum(jnp.where(lane == head, run_ref[...], 0.0), axis=-1, keepdims=True)
    length = jnp.zeros((total_rows, LANES), jnp.int32)
    for s in range(seqs):
        length = jnp.where(row // each == s, lengths_ref[s], length)
    length = length[:, 0:1]
    slot = lane_index((total_rows, past))
    gate = bias_rows_ref[...]
    last = jnp.sum(jnp.where(slot == length - 1, gate, 0.0), axis=-1, keepdims=True)
    scores = score_ref[...] * scale + (last - gate) + row_run
    scores = jnp.where(slot < length, scores, -jnp.inf)
    by_key = jnp.transpose(
        jnp.concatenate([run, jnp.zeros((LANES - rows, LANES), F32)], axis=0)
    )
    key_run = jnp.zeros((total_rows, LANES), F32)
    for h in range(heads):
        key_run = jnp.where(head == h, by_key[h : h + 1, :], key_run)
    fresh = dot_t(query, new_keys) * scale + row_run - key_run
    visible = (lane // new == row // each) & (lane % new <= row % new)
    fresh = jnp.where(visible, fresh, -jnp.inf)
    top = jnp.maximum(
        jnp.max(scores, axis=-1, keepdims=True), jnp.max(fresh, axis=-1, keepdims=True)
    )
    weights = jnp.exp(scores - top)
    fresh = jnp.exp(fresh - top)
    total = jnp.sum(weights, axis=-1, keepdims=True) + jnp.sum(fresh, axis=-1, keepdims=True)
    inverse = 1.0 / total
    weights = weights.astype(BF16)
    summed = jnp.dot(fresh.astype(BF16), new_values, preferred_element_type=F32)
    copies[6].wait()
    for s in range(seqs):
        part = slice(s * each, (s + 1) * each)
        attention = summed[part, :] + jnp.dot(
            weights[part, :], values_ref[s], preferred_element_type=F32
        )
        attention = attention * inverse[part, :]
        for h in range(heads):
            result_ref[s * new : (s + 1) * new, h * head_dim : (h + 1) * head_dim] = attention[
                h * new : (h + 1) * new, :
            ]
    copies[7].wait()
    out_ref[...] = jnp.dot(
        result_ref[...].astype(BF16), wo_ref[...], preferred_element_type=F32
    ).astype(BF16)


def decode(tokens, gain, wq, wk, wv, wg, bias, keys, values, gate, lengths, wo):
    seqs, new, model = tokens.shape
    heads = bias.shape[0]
    width, head_dim = wq.shape[1], wk.shape[1]
    past = keys.shape[1]
    each = heads * new
    hbm = pl.BlockSpec(memory_space=pl.ANY)
    vmem = pl.BlockSpec(memory_space=pltpu.VMEM)
    return pl.pallas_call(
        dec_kernel,
        out_shape=jax.ShapeDtypeStruct((seqs * new, wo.shape[1]), BF16),
        in_specs=[
            pl.BlockSpec(memory_space=pltpu.SMEM),
            hbm,
            vmem,
            hbm,
            hbm,
            hbm,
            vmem,
            vmem,
            hbm,
            hbm,
            hbm,
            hbm,
        ],
        out_specs=vmem,
        scratch_shapes=[
            pltpu.VMEM(wo.shape, BF16),
            pltpu.VMEM((seqs, new, model), BF16),
            pltpu.VMEM((model, width), BF16),
            pltpu.VMEM((model, head_dim), BF16),
            pltpu.VMEM((model, head_dim), BF16),
            pltpu.VMEM((seqs, past, head_dim), BF16),
            pltpu.VMEM((seqs, past, head_dim), BF16),
            pltpu.VMEM((seqs, heads, past), F32),
            pltpu.VMEM((seqs * new, model), F32),
            pltpu.VMEM((seqs * each, head_dim), F32),
            pltpu.VMEM((seqs * each, LANES), F32),
            pltpu.VMEM((seqs * each, past), F32),
            pltpu.VMEM((seqs * each, past), F32),
            pltpu.VMEM((seqs * new, width), F32),
            pltpu.SemaphoreType.DMA((8,)),
        ],
        cost_estimate=cost(6.0, 8 << 20),
        name="decode",
    )(
        lengths,
        tokens,
        gain.reshape(1, model),
        wq,
        wk,
        wv,
        wg.T,
        bias.reshape(1, heads),
        keys.reshape(seqs, past, head_dim),
        values.reshape(seqs, past, head_dim),
        gate,
        wo,
    )


def groups(sizes, cores):
    far = FAR
    deep, across = sizes[0] // far, sizes[1] // far
    alike, block = {}, {}
    for z in range(sizes[0]):
        for y in range(sizes[1]):
            for core in range(cores):
                index = (z * sizes[1] + y) * cores + core
                first = core % 2 == 0
                alike.setdefault((core, z // deep if first else y // across), []).append(index)
                block.setdefault(
                    (core, z % deep if first else y % across, y if first else z), []
                ).append(index)
    return far, list(alike.values()), list(block.values())


def exchange(x, members):
    return lax.all_to_all(
        x, PART, split_axis=0, concat_axis=0, axis_index_groups=members, tiled=True
    )


def swapped(x):
    return lax.ppermute(x, "tp", [(0, 1), (1, 0)])


def layer(
    piece_tokens,
    dec_tokens,
    norm_gain,
    query_weight,
    key_weight,
    value_weight,
    gate_weight,
    gate_bias,
    out_weight,
    out_gain,
    past_keys,
    past_values,
    past_gate,
    dec_keys,
    dec_values,
    dec_gate,
    dec_lengths,
):
    heads = gate_bias.shape[0]
    sizes = (lax.axis_size("z"), lax.axis_size("y"))
    far, alike, block = groups(sizes, lax.axis_size("tp"))
    near = sizes[0] * sizes[1] // far
    count, _, head_dim = past_keys.shape

    shares = piece_queries(piece_tokens, norm_gain, query_weight, gate_weight, gate_bias, near)
    shared = exchange(shares, alike)
    payload = block_payload(
        sizes,
        shared,
        piece_tokens,
        norm_gain,
        key_weight,
        value_weight,
        past_keys.reshape(count, head_dim),
        past_values.reshape(count, head_dim),
        past_gate,
        far,
    )
    new_blocks = exchange(payload, block)
    partials = attend(shared, new_blocks, heads, sizes)
    back = exchange(partials, alike)
    dec_partial = decode(
        dec_tokens,
        norm_gain,
        query_weight,
        key_weight,
        value_weight,
        gate_weight,
        gate_bias,
        dec_keys,
        dec_values,
        dec_gate,
        dec_lengths,
        out_weight,
    )
    dec_partial = jnp.pad(dec_partial, ((piece_tokens.shape[0], 0), (0, 0)))
    partial = merge(back, out_weight, dec_partial, heads)
    other = swapped(partial)
    return final(partial, other, out_gain, piece_tokens.shape, dec_tokens.shape)


def solution(mesh):
    finer = Mesh(
        mesh.devices.reshape(mesh.shape["dp"], 8, 8, mesh.shape["tp"]),
        ("dp", "z", "y", "tp"),
    )
    in_specs = (
        P(DP_KV, None),
        P(DP_KV, None, None),
        P(),
        P(None, "tp"),
        P(None, "tp"),
        P(None, "tp"),
        P(None, "tp"),
        P("tp"),
        P("tp", None),
        P(),
        P(DP_KV, "tp", None),
        P(DP_KV, "tp", None),
        P("tp", DP_KV),
        P(DP_KV, None, "tp", None),
        P(DP_KV, None, "tp", None),
        P(DP_KV, "tp", None),
        P(DP_KV),
    )
    out_specs = (P(DP_KV, None), P(DP_KV, None, None))
    return jax.shard_map(layer, mesh=finer, in_specs=in_specs, out_specs=out_specs, check_vma=False)
```

```python
import functools

import jax
import jax.numpy as jnp
from jax import lax
from jax.experimental import pallas as pl
from jax.experimental.pallas import tpu as pltpu
from jax.sharding import Mesh
from jax.sharding import PartitionSpec as P

PART = ("z", "y", "tp")
DP_KV = ("dp", "z", "y")
FAR = 4
EPS = 1e-06
LANES = 128
F32 = jnp.float32
BF16 = jnp.bfloat16
ROOM = 20 * 1024 * 1024


def rms_scale(source, scale_gain):
    widened = source.astype(F32)
    return (
        widened * lax.rsqrt(jnp.mean(widened * widened, axis=-1, keepdims=True) + EPS) * scale_gain
    )


def three_parts(x):
    high = x.astype(BF16).astype(F32)
    rest = x - high
    middle = rest.astype(BF16).astype(F32)
    low = (rest - middle).astype(BF16).astype(F32)
    return high, middle, low


def lane_index(shape):
    return lax.broadcasted_iota(jnp.int32, shape, len(shape) - 1)


def row_index(shape):
    return lax.broadcasted_iota(jnp.int32, shape, 0)


def pack_lanes(x, heads):
    high, middle, low = three_parts(x)
    lane = lane_index(x.shape)
    middle = pltpu.roll(middle, heads, 1)
    low = pltpu.roll(low, 2 * heads, 1)
    return jnp.where(
        lane < heads,
        high,
        jnp.where(lane < 2 * heads, middle, jnp.where(lane < 3 * heads, low, 0.0)),
    )


def unpack_lanes(x, heads):
    return x + pltpu.roll(x, LANES - heads, 1) + pltpu.roll(x, LANES - 2 * heads, 1)


def my_place(sizes, far):
    z, y, core = (lax.axis_index(name) for name in PART)
    deep, across = sizes[0] // far, sizes[1] // far
    first = core == 0
    return (
        jnp.where(first, z // deep, y // across),
        jnp.where(first, (z % deep) * sizes[1] + y, z * across + y % across),
        core,
    )


def fold_rows(x):
    half = x.shape[0] // 2
    upper, lower = x[0:half, :], x[half:, :]
    return jnp.where(lane_index(upper.shape) < 16, upper, pltpu.roll(lower, 16, 1))


def unfold_rows(x):
    return x, pltpu.roll(x, LANES - 16, 1)


def proj_kernel(
    heads,
    tok_hbm,
    gain_hbm,
    wq_hbm,
    wg_hbm,
    bias_hbm,
    share_ref,
    tok_ref,
    gain_ref,
    wq_ref,
    wg_ref,
    bias_ref,
    sems,
):
    model, width = wq_ref.shape
    pieces = sems.shape[0] - 4
    depth = model // pieces
    moves = [
        (tok_hbm, tok_ref),
        (gain_hbm, gain_ref),
        (wg_hbm, wg_ref),
        (bias_hbm, bias_ref),
    ]
    moves += [
        (wq_hbm.at[pl.ds(n * depth, depth)], wq_ref.at[pl.ds(n * depth, depth)])
        for n in range(pieces)
    ]
    copies = [pltpu.make_async_copy(src, dst, sems.at[n]) for n, (src, dst) in enumerate(moves)]
    for copy in copies:
        copy.start()
    for copy in copies[0:4]:
        copy.wait()
    normed = rms_scale(tok_ref[...], gain_ref[...]).astype(BF16)
    rows = normed.shape[0]
    logits = dot_t(normed, wg_ref[...]) + bias_ref[...]
    gates = jnp.minimum(logits, 0.0) - jnp.log1p(jnp.exp(-jnp.abs(logits)))
    lane = lane_index((rows, LANES))
    run = jnp.zeros((rows, LANES), F32)
    for h in range(heads):
        run = jnp.where(lane == h, gates[:, h : h + 1], run)
    row = row_index((rows, LANES))
    step = 1
    while step < rows:
        run = run + jnp.where(row >= step, pltpu.roll(run, step, 0), 0.0)
        step *= 2
    packed = fold_rows(pack_lanes(run, heads)).astype(BF16)
    queries = jnp.zeros((rows, width), F32)
    for n in range(pieces):
        copies[4 + n].wait()
        queries = queries + jnp.dot(
            normed[:, n * depth : (n + 1) * depth],
            wq_ref[n * depth : (n + 1) * depth, :],
            preferred_element_type=F32,
        )
    queries = queries.astype(BF16)
    head_dim = width // heads
    for slot in range(share_ref.shape[0]):
        for h in range(heads):
            share_ref[slot, h * rows : (h + 1) * rows, :] = queries[
                :, h * head_dim : (h + 1) * head_dim
            ]
        share_ref[slot, heads * rows :, :] = packed


def piece_queries(tokens, gain, wq, wg, bias, near):
    rows, model = tokens.shape
    heads = bias.shape[0]
    width = wq.shape[1]
    hbm = pl.BlockSpec(memory_space=pl.ANY)
    vmem = pl.BlockSpec(memory_space=pltpu.VMEM)
    return pl.pallas_call(
        functools.partial(proj_kernel, heads),
        out_shape=jax.ShapeDtypeStruct(
            (near, heads * rows + rows // 2, width // heads), BF16
        ),
        in_specs=[hbm] * 5,
        out_specs=vmem,
        scratch_shapes=[
            pltpu.VMEM((rows, model), BF16),
            pltpu.VMEM((1, model), F32),
            pltpu.VMEM((model, width), BF16),
            pltpu.VMEM((heads, model), BF16),
            pltpu.VMEM((1, heads), F32),
            pltpu.SemaphoreType.DMA((8,)),
        ],
        cost_estimate=cost(3.0, 2 << 20),
        name="piece_queries",
    )(tokens, gain.reshape(1, model), wq, wg.T, bias.reshape(1, heads))


def payload_kernel(
    heads,
    sizes,
    shared_ref,
    tok_ref,
    gain_ref,
    wk_ref,
    wv_ref,
    pk_ref,
    pv_ref,
    gate_ref,
    out_ref,
    parts_ref,
):
    rows = tok_ref.shape[0]
    near = shared_ref.shape[0]
    tail = heads * rows
    count = pk_ref.shape[0]
    normed = rms_scale(tok_ref[...], gain_ref[...]).astype(BF16)
    keys = jnp.dot(normed, wk_ref[...], preferred_element_type=F32).astype(BF16)
    values = jnp.dot(normed, wv_ref[...], preferred_element_type=F32).astype(BF16)
    my_near = my_place(sizes, out_ref.shape[0])[1]
    mine = shared_ref[my_near, tail:, :].astype(F32)
    run = jnp.concatenate(unfold_rows(mine), axis=0)
    totals = jnp.concatenate(
        [shared_ref[i, tail:, :].astype(F32)[rows // 2 - 1 : rows // 2, :] for i in range(near)],
        axis=0,
    )
    run = jnp.where(lane_index(run.shape) < 16, run, totals).astype(BF16)
    halves = count // LANES
    block = heads * halves
    parts_ref[...] = jnp.zeros_like(parts_ref)
    for n, part in enumerate(three_parts(gate_ref[...])):
        for half in range(halves):
            at = n * block + half * heads
            parts_ref[at : at + heads, :] = part[:, half * LANES : (half + 1) * LANES]
    parts = parts_ref[...].astype(BF16)
    first = 3 * rows
    for slot in range(out_ref.shape[0]):
        out_ref[slot, 0:rows, :] = keys
        out_ref[slot, rows : 2 * rows, :] = values
        out_ref[slot, 2 * rows : first, :] = run
        out_ref[slot, first : first + count, :] = pk_ref[...]
        out_ref[slot, first + count : first + 2 * count, :] = pv_ref[...]
        out_ref[slot, first + 2 * count :, :] = parts


def block_payload(sizes, shared, tokens, gain, wk, wv, past_keys, past_values, past_gate, far):
    rows, model = tokens.shape
    assert shared.shape[0] == rows
    count, head_dim = past_keys.shape
    heads = past_gate.shape[0]
    gate_rows = -(-3 * heads * (count // LANES) // 16) * 16
    vmem = pl.BlockSpec(memory_space=pltpu.VMEM)
    return pl.pallas_call(
        functools.partial(payload_kernel, heads, sizes),
        out_shape=jax.ShapeDtypeStruct(
            (far, 3 * rows + 2 * count + gate_rows, head_dim), BF16
        ),
        in_specs=[vmem] * 8,
        out_specs=vmem,
        scratch_shapes=[pltpu.VMEM((gate_rows, LANES), F32)],
        compiler_params=room(),
        cost_estimate=cost(2.0, 2 << 20),
        name="block_payload",
    )(
        shared,
        tokens,
        gain.reshape(1, model),
        wk,
        wv,
        past_keys,
        past_values,
        past_gate,
    )


def room():
    return pltpu.CompilerParams(vmem_limit_bytes=ROOM)


def cost(micros, moved):
    return pl.CostEstimate(
        flops=int(micros * 15e6), bytes_accessed=int(moved), transcendentals=0
    )


def dot_t(a, b):
    return lax.dot_general(a, b, (((1,), (1,)), ((), ())), preferred_element_type=F32)


def past_count(payload_rows, heads):
    count = LANES
    while 2 * count + -(-3 * heads * (count // LANES) // 16) * 16 < payload_rows:
        count += LANES
    return count


def attend_kernel(heads, sizes, shared_ref, new_ref, out_ref):
    near, tail = shared_ref.shape[0], shared_ref.shape[1] * (2 * heads) // (2 * heads + 1)
    rows = tail // heads
    far, head_dim = new_ref.shape[0], new_ref.shape[2]
    scale = head_dim ** (-0.5)
    my_far, my_near, core = my_place(sizes, far)
    across = sizes[1] // far

    def block_place(block, alike):
        by_z = block * near + alike
        by_y = (alike // across) * sizes[1] + block * across + alike % across
        return jnp.where(core == 0, by_z, by_y)

    folded = [
        unpack_lanes(new_ref[f, 2 * rows : 3 * rows, :].astype(F32), heads) for f in range(far)
    ]
    totals = pltpu.roll(jnp.concatenate(folded, axis=0), LANES - 16, 1)
    shape = (8 + near, far * near)
    row = row_index(shape)
    wanted = jnp.where(row < 8, block_place(row, my_near), block_place(my_far, row - 8))
    source = lane_index(shape)
    earlier = (block_place(source // near, source % near) < wanted).astype(F32)
    before = jnp.dot(
        earlier, totals, preferred_element_type=F32, precision=lax.Precision.HIGHEST
    )
    new_count = far * rows
    key_run = jnp.concatenate(
        [folded[f] + before[f : f + 1, :] for f in range(far)]
        + [jnp.zeros((LANES - new_count, LANES), F32)],
        axis=0,
    )
    key_run = jnp.transpose(key_run)
    half = rows // 2
    upper, lower = (
        unpack_lanes(x, heads)
        for x in unfold_rows(shared_ref[:, tail:, :].astype(F32).reshape(near * half, LANES))
    )
    row_runs = []
    for i in range(near):
        start = before[8 + i : 9 + i, :]
        row_runs.append(upper[i * half : (i + 1) * half, :] + start)
        row_runs.append(lower[i * half : (i + 1) * half, :] + start)
    row_run = jnp.concatenate(row_runs, axis=0)
    shape = (near * rows, LANES)
    row = row_index(shape)
    row_place = block_place(my_far, row // rows) * rows + row % rows
    lane = lane_index(shape)
    key_place = block_place(lane // rows, my_near) * rows + lane % rows
    visible = (key_place <= row_place) & (lane < new_count)
    new_keys = jnp.concatenate(
        [new_ref[f, 0:rows, :] for f in range(far)]
        + [jnp.zeros((LANES - new_count, head_dim), BF16)],
        axis=0,
    )
    new_values = jnp.concatenate(
        [new_ref[f, rows : 2 * rows, :] for f in range(far)]
        + [jnp.zeros((LANES - new_count, head_dim), BF16)],
        axis=0,
    )
    first = 3 * rows
    count = past_count(new_ref.shape[1] - first, heads)
    halves = count // LANES
    block = heads * halves
    gates = []
    for f in range(far):
        parts = new_ref[f, first + 2 * count :, :].astype(F32)
        gates.append(parts[0:block] + parts[block : 2 * block] + parts[2 * block : 3 * block])
    lse_lanes = jnp.zeros(shape, F32)
    for h in range(heads):
        query = shared_ref[:, h * rows : (h + 1) * rows, :].reshape(near * rows, head_dim)
        scores = []
        for f in range(far):
            row = jnp.concatenate(
                [gates[f][half * heads + h : half * heads + h + 1, :] for half in range(halves)],
                axis=1,
            )
            scores.append(dot_t(query, new_ref[f, first : first + count, :]) * scale + row)
        fresh = dot_t(query, new_keys) * scale - key_run[h : h + 1, :]
        fresh = jnp.where(visible, fresh, -jnp.inf)
        top = jnp.maximum(
            jnp.max(functools.reduce(jnp.maximum, scores), axis=-1, keepdims=True),
            jnp.max(fresh, axis=-1, keepdims=True),
        )
        fresh = jnp.exp(fresh - top)
        summed = jnp.dot(fresh.astype(BF16), new_values, preferred_element_type=F32)
        wide = jnp.zeros(scores[0].shape, F32)
        for f in range(far):
            exponent = jnp.exp(scores[f] - top)
            wide = wide + exponent
            summed = summed + jnp.dot(
                exponent.astype(BF16),
                new_ref[f, first + count : first + 2 * count, :],
                preferred_element_type=F32,
            )
        total = jnp.sum(wide, axis=-1, keepdims=True) + jnp.sum(fresh, axis=-1, keepdims=True)
        result = (summed * (1.0 / total)).astype(BF16)
        out_ref[:, h * rows : (h + 1) * rows, :] = result.reshape(near, rows, head_dim)
        lse_lanes = jnp.where(lane == h, top + jnp.log(total), lse_lanes)
    lse_lanes = lse_lanes + jnp.where(lane < heads, row_run, 0.0)
    packed = pack_lanes(lse_lanes, heads).reshape(near, 2, half, LANES)
    folded = jnp.where(
        lane_index((near * half, LANES)) < 16,
        packed[:, 0].reshape(near * half, LANES),
        pltpu.roll(packed[:, 1].reshape(near * half, LANES), 16, 1),
    )
    out_ref[:, tail:, :] = folded.astype(BF16).reshape(near, half, LANES)


def attend(shared, new_blocks, heads, sizes):
    vmem = pl.BlockSpec(memory_space=pltpu.VMEM)
    return pl.pallas_call(
        functools.partial(attend_kernel, heads, sizes),
        out_shape=jax.ShapeDtypeStruct(shared.shape, BF16),
        in_specs=[vmem, vmem],
        out_specs=vmem,
        compiler_params=room(),
        cost_estimate=cost(4.0, 1 << 20),
        name="attend",
    )(shared, new_blocks)


def merge_kernel(heads, back_ref, wo_ref, dec_ref, out_ref):
    near, tail = back_ref.shape[0], back_ref.shape[1] * (2 * heads) // (2 * heads + 1)
    rows = tail // heads
    half = rows // 2
    head_dim = back_ref.shape[2]
    upper, lower = (
        unpack_lanes(x, heads)
        for x in unfold_rows(back_ref[:, tail:, :].astype(F32).reshape(near * half, LANES))
    )
    blocks = [
        jnp.concatenate([x[i * half : (i + 1) * half, :] for x in (upper, lower)], axis=0)
        for i in range(near)
    ]
    top = functools.reduce(jnp.maximum, blocks)
    weights = [jnp.exp(b - top) for b in blocks]
    inverse = 1.0 / functools.reduce(jnp.add, weights)
    weights = [w * inverse for w in weights]
    merged = []
    for h in range(heads):
        summed = jnp.zeros((rows, head_dim), F32)
        for i in range(near):
            part = back_ref[i, h * rows : (h + 1) * rows, :].astype(F32)
            summed = summed + part * weights[i][:, h : h + 1]
        merged.append(summed.astype(BF16))
    attention = jnp.concatenate(merged, axis=1)
    out_ref[0:rows, :] = jnp.dot(
        attention, wo_ref[...], preferred_element_type=F32
    ).astype(BF16)
    out_ref[rows:, :] = dec_ref[rows:, :]


def merge(back, out_weight, dec_partial, heads):
    vmem = pl.BlockSpec(memory_space=pltpu.VMEM)
    return pl.pallas_call(
        functools.partial(merge_kernel, heads),
        out_shape=jax.ShapeDtypeStruct(
            (dec_partial.shape[0], out_weight.shape[1]), BF16
        ),
        in_specs=[vmem, vmem, vmem],
        out_specs=vmem,
        compiler_params=room(),
        cost_estimate=cost(2.0, 2 << 20),
        name="merge",
    )(back, out_weight, dec_partial)


def final_kernel(one_ref, two_ref, gain_ref, piece_ref, dec_ref, held_ref):
    mixed = one_ref[...].astype(F32) + two_ref[...].astype(F32)
    rows = rms_scale(mixed, gain_ref[...])
    count, new = piece_ref.shape[0], dec_ref.shape[1]
    piece_ref[...] = rows[0:count, :].astype(BF16)
    held_ref[...] = rows[count:, :]
    for s in range(dec_ref.shape[0]):
        dec_ref[s] = held_ref[s * new : (s + 1) * new, :].astype(BF16)


def final(one, two, gain, piece_shape, dec_shape):
    vmem = pl.BlockSpec(memory_space=pltpu.VMEM)
    return pl.pallas_call(
        final_kernel,
        out_shape=(
            jax.ShapeDtypeStruct(piece_shape, BF16),
            jax.ShapeDtypeStruct(dec_shape, BF16),
        ),
        in_specs=[vmem] * 3,
        out_specs=(vmem, vmem),
        scratch_shapes=[pltpu.VMEM((one.shape[0] - piece_shape[0], one.shape[1]), F32)],
        compiler_params=room(),
        cost_estimate=cost(0.5, 1 << 17),
        name="final",
    )(one, two, gain.reshape(1, -1))


def dec_kernel(
    lengths_ref,
    tok_hbm,
    gain_ref,
    wq_hbm,
    wk_hbm,
    wv_hbm,
    wg_ref,
    bias_ref,
    keys_hbm,
    values_hbm,
    gate_hbm,
    wo_hbm,
    out_ref,
    wo_ref,
    tok_ref,
    wq_ref,
    wk_ref,
    wv_ref,
    keys_ref,
    values_ref,
    gate_ref,
    rows_ref,
    query_ref,
    run_ref,
    bias_rows_ref,
    score_ref,
    result_ref,
    sems,
):
    seqs, new, _ = tok_ref.shape
    width = wq_ref.shape[1]
    past, head_dim = keys_ref.shape[1], keys_ref.shape[2]
    heads = width // head_dim
    scale = head_dim ** (-0.5)
    each = heads * new
    total_rows = seqs * each
    moves = (
        (tok_hbm, tok_ref),
        (wq_hbm, wq_ref),
        (wk_hbm, wk_ref),
        (wv_hbm, wv_ref),
        (gate_hbm, gate_ref),
        (keys_hbm, keys_ref),
        (values_hbm, values_ref),
        (wo_hbm, wo_ref),
    )
    copies = [pltpu.make_async_copy(src, dst, sems.at[n]) for n, (src, dst) in enumerate(moves)]
    for copy in copies:
        copy.start()
    copies[0].wait()
    for s in range(seqs):
        rows_ref[s * new : (s + 1) * new, :] = tok_ref[s].astype(F32)
    normed = rms_scale(rows_ref[...], gain_ref[...]).astype(BF16)
    rows = seqs * new
    logits = dot_t(normed, wg_ref[...]) + bias_ref[...]
    gates = jnp.minimum(logits, 0.0) - jnp.log1p(jnp.exp(-jnp.abs(logits)))
    lane = lane_index((rows, LANES))
    row = row_index((rows, LANES))
    run = jnp.zeros((rows, LANES), F32)
    for h in range(heads):
        run = jnp.where(lane == h, gates[:, h : h + 1], run)
    step = 1
    while step < new:
        run = run + jnp.where(row % new >= step, pltpu.roll(run, step, 0), 0.0)
        step *= 2
    copies[1].wait()
    queries = jnp.dot(normed, wq_ref[...], preferred_element_type=F32)
    copies[2].wait()
    pad = jnp.zeros((LANES - rows, head_dim), BF16)
    new_keys = jnp.dot(normed, wk_ref[...], preferred_element_type=F32).astype(BF16)
    copies[3].wait()
    new_values = jnp.dot(normed, wv_ref[...], preferred_element_type=F32).astype(BF16)
    new_keys = jnp.concatenate([new_keys, pad], axis=0)
    new_values = jnp.concatenate([new_values, pad], axis=0)
    copies[4].wait()
    for s in range(seqs):
        for h in range(heads):
            at = s * each + h * new
            query_ref[at : at + new, :] = queries[
                s * new : (s + 1) * new, h * head_dim : (h + 1) * head_dim
            ]
            run_ref[at : at + new, :] = run[s * new : (s + 1) * new, :]
            bias_rows_ref[at : at + new, :] = jnp.broadcast_to(
                gate_ref[s, h : h + 1, :], (new, past)
            )
    query = query_ref[...].astype(BF16)
    copies[5].wait()
    for s in range(seqs):
        score_ref[s * each : (s + 1) * each, :] = dot_t(
            query[s * each : (s + 1) * each, :], keys_ref[s]
        )
    lane = lane_index((total_rows, LANES))
    row = row_index((total_rows, LANES))
    head = (row // new) % heads
    row_run = jnp.sum(jnp.where(lane == head, run_ref[...], 0.0), axis=-1, keepdims=True)
    length = jnp.zeros((total_rows, LANES), jnp.int32)
    for s in range(seqs):
        length = jnp.where(row // each == s, lengths_ref[s], length)
    length = length[:, 0:1]
    slot = lane_index((total_rows, past))
    gate = bias_rows_ref[...]
    last = jnp.sum(jnp.where(slot == length - 1, gate, 0.0), axis=-1, keepdims=True)
    scores = score_ref[...] * scale + (last - gate) + row_run
    scores = jnp.where(slot < length, scores, -jnp.inf)
    by_key = jnp.transpose(
        jnp.concatenate([run, jnp.zeros((LANES - rows, LANES), F32)], axis=0)
    )
    key_run = jnp.zeros((total_rows, LANES), F32)
    for h in range(heads):
        key_run = jnp.where(head == h, by_key[h : h + 1, :], key_run)
    fresh = dot_t(query, new_keys) * scale + row_run - key_run
    visible = (lane // new == row // each) & (lane % new <= row % new)
    fresh = jnp.where(visible, fresh, -jnp.inf)
    top = jnp.maximum(
        jnp.max(scores, axis=-1, keepdims=True), jnp.max(fresh, axis=-1, keepdims=True)
    )
    weights = jnp.exp(scores - top)
    fresh = jnp.exp(fresh - top)
    total = jnp.sum(weights, axis=-1, keepdims=True) + jnp.sum(fresh, axis=-1, keepdims=True)
    inverse = 1.0 / total
    weights = weights.astype(BF16)
    summed = jnp.dot(fresh.astype(BF16), new_values, preferred_element_type=F32)
    copies[6].wait()
    for s in range(seqs):
        part = slice(s * each, (s + 1) * each)
        attention = summed[part, :] + jnp.dot(
            weights[part, :], values_ref[s], preferred_element_type=F32
        )
        attention = attention * inverse[part, :]
        for h in range(heads):
            result_ref[s * new : (s + 1) * new, h * head_dim : (h + 1) * head_dim] = attention[
                h * new : (h + 1) * new, :
            ]
    copies[7].wait()
    out_ref[...] = jnp.dot(
        result_ref[...].astype(BF16), wo_ref[...], preferred_element_type=F32
    ).astype(BF16)


def decode(tokens, gain, wq, wk, wv, wg, bias, keys, values, gate, lengths, wo):
    seqs, new, model = tokens.shape
    heads = bias.shape[0]
    width, head_dim = wq.shape[1], wk.shape[1]
    past = keys.shape[1]
    each = heads * new
    hbm = pl.BlockSpec(memory_space=pl.ANY)
    vmem = pl.BlockSpec(memory_space=pltpu.VMEM)
    return pl.pallas_call(
        dec_kernel,
        out_shape=jax.ShapeDtypeStruct((seqs * new, wo.shape[1]), BF16),
        in_specs=[
            pl.BlockSpec(memory_space=pltpu.SMEM),
            hbm,
            vmem,
            hbm,
            hbm,
            hbm,
            vmem,
            vmem,
            hbm,
            hbm,
            hbm,
            hbm,
        ],
        out_specs=vmem,
        scratch_shapes=[
            pltpu.VMEM(wo.shape, BF16),
            pltpu.VMEM((seqs, new, model), BF16),
            pltpu.VMEM((model, width), BF16),
            pltpu.VMEM((model, head_dim), BF16),
            pltpu.VMEM((model, head_dim), BF16),
            pltpu.VMEM((seqs, past, head_dim), BF16),
            pltpu.VMEM((seqs, past, head_dim), BF16),
            pltpu.VMEM((seqs, heads, past), F32),
            pltpu.VMEM((seqs * new, model), F32),
            pltpu.VMEM((seqs * each, head_dim), F32),
            pltpu.VMEM((seqs * each, LANES), F32),
            pltpu.VMEM((seqs * each, past), F32),
            pltpu.VMEM((seqs * each, past), F32),
            pltpu.VMEM((seqs * new, width), F32),
            pltpu.SemaphoreType.DMA((8,)),
        ],
        cost_estimate=cost(6.0, 8 << 20),
        name="decode",
    )(
        lengths,
        tokens,
        gain.reshape(1, model),
        wq,
        wk,
        wv,
        wg.T,
        bias.reshape(1, heads),
        keys.reshape(seqs, past, head_dim),
        values.reshape(seqs, past, head_dim),
        gate,
        wo,
    )


def groups(sizes, cores):
    far = FAR
    deep, across = sizes[0] // far, sizes[1] // far
    alike, block = {}, {}
    for z in range(sizes[0]):
        for y in range(sizes[1]):
            for core in range(cores):
                index = (z * sizes[1] + y) * cores + core
                first = core % 2 == 0
                alike.setdefault((core, z // deep if first else y // across), []).append(index)
                block.setdefault(
                    (core, z % deep if first else y % across, y if first else z), []
                ).append(index)
    return far, list(alike.values()), list(block.values())


def exchange(x, members):
    return lax.all_to_all(
        x, PART, split_axis=0, concat_axis=0, axis_index_groups=members, tiled=True
    )


def swapped(x):
    return lax.ppermute(x, "tp", [(0, 1), (1, 0)])


def layer(
    piece_tokens,
    dec_tokens,
    norm_gain,
    query_weight,
    key_weight,
    value_weight,
    gate_weight,
    gate_bias,
    out_weight,
    out_gain,
    past_keys,
    past_values,
    past_gate,
    dec_keys,
    dec_values,
    dec_gate,
    dec_lengths,
):
    heads = gate_bias.shape[0]
    sizes = (lax.axis_size("z"), lax.axis_size("y"))
    far, alike, block = groups(sizes, lax.axis_size("tp"))
    near = sizes[0] * sizes[1] // far
    count, _, head_dim = past_keys.shape

    shares = piece_queries(piece_tokens, norm_gain, query_weight, gate_weight, gate_bias, near)
    shared = exchange(shares, alike)
    payload = block_payload(
        sizes,
        shared,
        piece_tokens,
        norm_gain,
        key_weight,
        value_weight,
        past_keys.reshape(count, head_dim),
        past_values.reshape(count, head_dim),
        past_gate,
        far,
    )
    new_blocks = exchange(payload, block)
    partials = attend(shared, new_blocks, heads, sizes)
    back = exchange(partials, alike)
    dec_partial = decode(
        dec_tokens,
        norm_gain,
        query_weight,
        key_weight,
        value_weight,
        gate_weight,
        gate_bias,
        dec_keys,
        dec_values,
        dec_gate,
        dec_lengths,
        out_weight,
    )
    dec_partial = jnp.pad(dec_partial, ((piece_tokens.shape[0], 0), (0, 0)))
    partial = merge(back, out_weight, dec_partial, heads)
    other = swapped(partial)
    return final(partial, other, out_gain, piece_tokens.shape, dec_tokens.shape)


def solution(mesh):
    finer = Mesh(
        mesh.devices.reshape(mesh.shape["dp"], 8, 8, mesh.shape["tp"]),
        ("dp", "z", "y", "tp"),
    )
    in_specs = (
        P(DP_KV, None),
        P(DP_KV, None, None),
        P(),
        P(None, "tp"),
        P(None, "tp"),
        P(None, "tp"),
        P(None, "tp"),
        P("tp"),
        P("tp", None),
        P(),
        P(DP_KV, "tp", None),
        P(DP_KV, "tp", None),
        P("tp", DP_KV),
        P(DP_KV, None, "tp", None),
        P(DP_KV, None, "tp", None),
        P(DP_KV, "tp", None),
        P(DP_KV),
    )
    out_specs = (P(DP_KV, None), P(DP_KV, None, None))
    return jax.shard_map(layer, mesh=finer, in_specs=in_specs, out_specs=out_specs, check_vma=False)
```
